512 devices in a mesh: sp: 16 (over z), fs: 4 (over y), tp: 8 (over x, core).
Axes of the slice: x: 4, y: 4, z: 16, core: 2. Of those that a mesh axis runs over, the one named last changes fastest.
Arguments:
- tokens: bfloat16 [8, 8192, 2048], P('fs', ('sp', 'tp')), may hold values from -6 to 6
- norm_gain: float32 [2048], replicated, may hold values from 0.1 to 1.9
- w_pool_in: bfloat16 [2048, 1024], P('fs', 'tp'), may hold values from -0.125 to 0.125
- pool_mix: bfloat16 [8, 128, 128], replicated, may hold values from -0.5 to 0.5
- pool_scale: float32 [1024], replicated, may hold values from 0.1 to 1.9
- w_query: bfloat16 [2048, 1024], P('fs', 'tp'), may hold values from -0.13258252 to 0.13258252
- w_key: bfloat16 [2048, 1024], P('fs', 'tp'), may hold values from -0.508233 to 0.508233
- w_value: bfloat16 [2048, 1024], P('fs', 'tp'), may hold values from -0.125 to 0.125
- gate_cache: float32 [8, 8, 8192], P('fs', 'tp'), may hold values from -1026 to 0, as said below
- w_out_pool: bfloat16 [1024, 2048], P('tp', 'fs'), may hold values from -0.125 to 0.125
- w_out_attn: bfloat16 [1024, 2048], P('tp', 'fs'), may hold values from -0.75 to 0.75
Outputs:
- mixed: bfloat16 [8, 8192, 2048], P('fs', ('sp', 'tp'))
The draws below stay inside these ranges and needn't reach their ends.
Inputs may be any that keep to these rules, and one draw needn't show every extreme that they name: `gate_cache`: each head's values never rise along the positions.
All inputs are finite; a program needn't handle non-finite values.
Results may differ from the reference program's by a relative error of at most 0.014.
Values may be sent and summed in bfloat16 or wider, within the bound.
No kernel may reach another device: no remote copies, remote signals or barrier semaphores. Data moves between devices by JAX's collectives and lax.ppermute only.
A program may use at most 128 MiB of HBM per device.

```python
import jax
import jax.numpy as jnp
from jax import lax

D = 2048
HEAD_DIM = 128
HEAD_TOTAL = 8
GROUPS = 8
GROUP_WIDTH = 128
POOL_WIDTH = 1024
ATTN_WIDTH = 1024
TOK_DEV = 512
SEQUENCE_LENGTH = 8192
SEQUENCE_TOTAL = 8
N_TP = 8


def query_key_pair(key):
    joined = jax.random.fold_in(key, 4242)
    first_key, second_key = jax.random.split(joined)
    query_part = jnp.clip(jax.random.normal(first_key, (D, ATTN_WIDTH), jnp.float32), -6.0, 6.0)
    key_part = jnp.clip(jax.random.normal(second_key, (D, ATTN_WIDTH), jnp.float32), -6.0, 6.0)
    return (query_part * D ** (-0.5), key_part * D ** (-0.5))


def draw_w_query(key, part):
    return query_key_pair(key)[0].astype(jnp.bfloat16)


def draw_w_key(key, part):
    return query_key_pair(key)[1].astype(jnp.bfloat16)


def draw_gate_cache(key, part):
    joined = jax.random.fold_in(key, 917)
    sequence_flows = jax.random.split(joined, 7)
    block_count = SEQUENCE_LENGTH // TOK_DEV
    ranking = jax.vmap(lambda single: jax.random.permutation(single, HEAD_TOTAL))(jax.random.split(sequence_flows[0], SEQUENCE_TOTAL))
    fast_count = HEAD_TOTAL // 2
    rapid_decay = ranking < fast_count
    quick_rate = jnp.exp(jax.random.uniform(sequence_flows[1], (SEQUENCE_TOTAL, HEAD_TOTAL), jnp.float32, jnp.log(1.0 / 100.0), jnp.log(1.0 / 30.0)))
    slow_total = jnp.exp(jax.random.uniform(sequence_flows[2], (SEQUENCE_TOTAL, HEAD_TOTAL), jnp.float32, jnp.log(0.15), jnp.log(0.5)))
    baseline_rate = jnp.where(rapid_decay, quick_rate, slow_total / SEQUENCE_LENGTH)
    block_factor = jnp.exp(jax.random.uniform(sequence_flows[3], (SEQUENCE_TOTAL, HEAD_TOTAL, block_count), jnp.float32, jnp.log(0.5), jnp.log(2.0)))
    position_multiplier = jnp.repeat(block_factor, TOK_DEV, axis=2)
    jitter_level = jax.random.uniform(sequence_flows[4], (SEQUENCE_TOTAL, HEAD_TOTAL, SEQUENCE_LENGTH), jnp.float32, 0.2, 1.8)
    spike_locations = jax.random.randint(sequence_flows[5], (SEQUENCE_TOTAL, HEAD_TOTAL, 2), 0, SEQUENCE_LENGTH)
    spike_depth = jax.random.uniform(sequence_flows[6], (SEQUENCE_TOTAL, HEAD_TOTAL, 2), jnp.float32, 0.22, 0.6)
    token_positions = jnp.arange(SEQUENCE_LENGTH)
    spike_hits = token_positions[None, None, None, :] == spike_locations[:, :, :, None]
    spike_events = jnp.sum(jnp.where(spike_hits, spike_depth[:, :, :, None], 0.0), axis=2)
    spike_events = jnp.where(rapid_decay[:, :, None], 0.0, spike_events)
    step_increments = baseline_rate[:, :, None] * position_multiplier * jitter_level + spike_events
    return -jnp.cumsum(step_increments, axis=2)


def block_scale(own_key, extent, shards, smallest, top_value):
    def one(dim, shards_of):
        steps = jax.random.uniform(jax.random.fold_in(jax.random.fold_in(own_key, 6), dim), (shards_of,), jnp.float32, smallest / len(shards), top_value / len(shards))
        return jnp.repeat(jnp.exp(steps), extent[dim] // shards_of).reshape((-1,) + (1,) * (len(extent) - dim - 1))

    gain = one(*shards[0])
    for cut in shards[1:]:
        gain = gain * one(*cut)
    return gain


def centred(rng, extent, scale, most, cuts=(), kind=jnp.bfloat16):
    result = jax.random.normal(rng, extent, jnp.float32) * scale
    if len(cuts) > 0:
        result = block_scale(rng, extent, cuts, -0.22, 0.18) * result
    return jnp.clip(result, min=-most, max=most).astype(kind)


def setup_inputs(seed: int = 0) -> dict:
    key_of = jax.random.split(jax.random.key(seed), 12)
    return {
        "tokens": centred(key_of[0], (SEQUENCE_TOTAL, SEQUENCE_LENGTH, D), 1.0, 6.0, ((0, 4), (1, 128))),
        "norm_gain": jnp.clip(1.0 + 0.18 * jax.random.normal(key_of[1], (D,), jnp.float32), 0.1, 1.9),
        "w_pool_in": centred(key_of[2], (D, POOL_WIDTH), D ** -0.5, 0.125, ((0, 4), (1, 8))),
        "pool_mix": centred(key_of[3], (GROUPS, GROUP_WIDTH, GROUP_WIDTH), GROUP_WIDTH ** -0.5, 0.5),
        "pool_scale": jnp.clip(1.0 + 0.18 * jax.random.normal(key_of[4], (POOL_WIDTH,), jnp.float32), 0.1, 1.9),
        "w_query": draw_w_query(jax.random.fold_in(key_of[11], 71), 0),
        "w_key": draw_w_key(jax.random.fold_in(key_of[11], 71), 0),
        "w_value": centred(key_of[7], (D, ATTN_WIDTH), D ** -0.5, 0.125, ((0, 4), (1, 8))),
        "gate_cache": draw_gate_cache(jax.random.fold_in(key_of[11], 71), 0),
        "w_out_pool": centred(key_of[9], (POOL_WIDTH, D), (POOL_WIDTH + ATTN_WIDTH) ** -0.5, 0.125, ((0, 8), (1, 4))),
        "w_out_attn": centred(key_of[10], (ATTN_WIDTH, D), (ATTN_WIDTH // 16) ** -0.5, 0.75, ((0, 8), (1, 4))),
    }


norm_eps = 1e-06
widest = 16

def settle(values):
    return lax.optimization_barrier(values.astype(jnp.bfloat16))

def window_sums(extended):
    outcome = []
    current = extended
    offset = 1
    for doubling in range(4):
        padding = jnp.zeros((offset, extended.shape[1]), extended.dtype)
        current = current + jnp.concatenate([padding, current[:-offset]], axis=0)
        offset = offset * 2
        outcome.append(current[widest - 1:])
    return outcome

def pool_branch(projected, mixing, scaling):
    row_count = projected.shape[0]
    channels = projected.shape[1]
    border = jnp.zeros((widest - 1, channels), jnp.float32)
    widened = projected.astype(jnp.float32)
    totals = window_sums(jnp.concatenate([border, widened], axis=0))
    token_positions = jnp.arange(row_count)
    window_index = jnp.arange(channels) // GROUP_WIDTH % 4
    averaged = jnp.zeros((row_count, channels), jnp.float32)
    for doubling in range(4):
        counted = jnp.minimum(token_positions + 1, 2 ** (doubling + 1)).astype(jnp.float32)
        picked = (window_index == doubling).astype(jnp.float32)
        averaged = averaged + picked[None, :] * totals[doubling] / counted[:, None]
    departure = settle(averaged - widened).astype(jnp.float32)
    mixed_rows = jnp.einsum('tgc,gcd->tgd', departure.reshape(row_count, GROUPS, GROUP_WIDTH), mixing.astype(jnp.float32))
    return (mixed_rows.reshape(row_count, channels) * scaling[None, :]).astype(jnp.bfloat16)

def attention(query_proj, key_proj, value_proj, gate_rows):
    row_count = query_proj.shape[0]
    block_rows = 512 if row_count % 512 == 0 else row_count
    shaped = (row_count, HEAD_TOTAL, HEAD_DIM)
    query_heads = query_proj.reshape(shaped).astype(jnp.float32)
    key_heads = key_proj.reshape(shaped).astype(jnp.float32)
    value_heads = value_proj.reshape(shaped).astype(jnp.float32)
    gate_cols = jnp.transpose(gate_rows)
    pieces = []
    for query_start in range(0, row_count, block_rows):
        query_end = query_start + block_rows
        scores = jnp.einsum('qhd,khd->qhk', query_heads[query_start:query_end], key_heads[:query_end]) * HEAD_DIM ** (-0.5)
        scores = scores + gate_cols[query_start:query_end, :, None] - gate_rows[None, :, :query_end]
        allowed = (jnp.arange(query_end)[None, :] <= jnp.arange(query_start, query_end)[:, None])[:, None, :]
        scores = jnp.where(allowed, scores, -jnp.inf)
        highest = lax.optimization_barrier(jnp.max(scores, axis=2, keepdims=True))
        lifted = jnp.exp(scores - highest)
        denominator = lax.optimization_barrier(jnp.sum(lifted, axis=2))
        rounded = settle(lifted).astype(jnp.float32)
        weighted = jnp.einsum('qhk,khd->qhd', rounded, value_heads[:query_end])
        pieces.append((weighted / denominator[:, :, None]).astype(jnp.bfloat16))
    return jnp.concatenate(pieces, axis=0).reshape(row_count, HEAD_TOTAL * HEAD_DIM)

def reference(tokens, norm_gain, w_pool_in, pool_mix, pool_scale, w_query, w_key, w_value, gate_cache, w_out_pool, w_out_attn):
    pool_share = POOL_WIDTH // N_TP
    attn_share = ATTN_WIDTH // N_TP
    outputs = []
    for sequence in range(SEQUENCE_TOTAL):
        widened = tokens[sequence].astype(jnp.float32)
        normed = (widened * lax.rsqrt(lax.optimization_barrier(jnp.mean(widened * widened, axis=-1, keepdims=True)) + norm_eps) * norm_gain[None, :]).astype(jnp.bfloat16)
        pool_in = settle(jnp.dot(normed, w_pool_in, preferred_element_type=jnp.float32))
        query_proj = settle(jnp.dot(normed, w_query, preferred_element_type=jnp.float32))
        key_proj = settle(jnp.dot(normed, w_key, preferred_element_type=jnp.float32))
        value_proj = settle(jnp.dot(normed, w_value, preferred_element_type=jnp.float32))
        pool_out = pool_branch(pool_in, pool_mix, pool_scale)
        attn_out = attention(query_proj, key_proj, value_proj, gate_cache[sequence])
        summed = jnp.zeros((SEQUENCE_LENGTH, D), jnp.float32)
        for member in range(N_TP):
            pool_lo = member * pool_share
            attn_lo = member * attn_share
            partial_value = jnp.dot(pool_out[:, pool_lo:pool_lo + pool_share], w_out_pool[pool_lo:pool_lo + pool_share], preferred_element_type=jnp.float32)
            partial_value = partial_value + jnp.dot(attn_out[:, attn_lo:attn_lo + attn_share], w_out_attn[attn_lo:attn_lo + attn_share], preferred_element_type=jnp.float32)
            summed = summed + settle(partial_value).astype(jnp.float32)
        outputs.append(summed.astype(jnp.bfloat16))
    return jnp.stack(outputs, axis=0)
```

```python
import jax
import jax.numpy as jnp
from jax import lax
from jax.experimental import pallas as pl
from jax.experimental.pallas import tpu as pltpu
from jax.sharding import Mesh
from jax.sharding import PartitionSpec as P

HD = 128
TP = ("tp_0", "tp_1")
SP_TP = ("sp", "tp_0", "tp_1")
EPS = 1e-06
MASKED = -1e30
LOG2E = 1.4426950408889634
F32 = jnp.float32
BF16 = jnp.bfloat16
VMEM_LIMIT = 56 * 1024 * 1024


def params(**kw):
    return pltpu.CompilerParams(vmem_limit_bytes=VMEM_LIMIT, **kw)


def whole(memory=pltpu.VMEM):
    return pl.BlockSpec(memory_space=memory)


def spread(x, axis):
    n = lax.axis_size(axis)
    return lax.all_to_all(jnp.broadcast_to(x[None], (n,) + x.shape), axis, 0, 0, tiled=True)


def sibling(x):
    return lax.ppermute(x, "tp_1", [(0, 1), (1, 0)])


def ring_of_four(x, axis):
    up = [(i, (i + 1) % 4) for i in range(4)]
    down = [(i, (i - 1) % 4) for i in range(4)]
    before = lax.ppermute(x, axis, up)
    after = lax.ppermute(x, axis, down)
    half = x.shape[0] // 2
    far_low = lax.ppermute(before[:half], axis, up)
    far_high = lax.ppermute(after[half:], axis, down)
    return x, before, after, far_low, far_high


def rms(x):
    wide = x.astype(F32)
    return lax.rsqrt(jnp.mean(wide * wide, axis=-1, keepdims=True) + EPS)


def factors_of(rows_of):
    seqs, rows, _ = rows_of[0].shape

    def body(x0, x1, x2, x3, x4, out_ref):
        at = 0
        for ref in (x0, x1, x2, x3, x4):
            for i in range(ref.shape[0]):
                out_ref[at : at + rows] = rms(ref[i])
                at += rows

    return pl.pallas_call(
        body,
        in_specs=[whole()] * 5,
        out_specs=whole(),
        out_shape=jax.ShapeDtypeStruct((4 * seqs * rows, 1), F32),
        compiler_params=params(),
        name="factors",
    )(*rows_of)


def project(places, norm, rows_of, own, other, half, factors, split):
    seqs, rows, depth = rows_of[0].shape
    kinds = len(factors)

    def body(p_ref, norm_ref, x0, x1, x2, x3, x4, own_ref, other_ref, *outs):
        x = jnp.concatenate(
            [x0[0], x0[1], x1[0], x1[1], x2[0], x2[1], x3[0], x4[0]], axis=0
        )
        r = norm_ref[...]
        for ref, head in ((own_ref, p_ref[0]), (other_ref, 1 - p_ref[0])):
            y = jnp.dot(x, ref[...], preferred_element_type=F32) * r
            for kind, factor in enumerate(factors):
                part = y[:, kind * HD : (kind + 1) * HD]
                if factor != 1.0:
                    part = part * factor
                part = part.astype(BF16)
                for a in range(4):
                    for i in range(seqs):
                        at = (a * seqs + i) * rows
                        if split:
                            outs[a][kind, 0, i, head] = part[at : at + rows]
                        else:
                            outs[0][p_ref[1 + a], i, head, kind] = part[at : at + rows]

    w_spec = pl.BlockSpec((depth, kinds * HD), lambda *_: (0, half))
    if split:
        shapes = [(kinds, 1, seqs, 2, rows, HD)] * 4
    else:
        shapes = [(4, seqs, 2, kinds, rows, HD)]
    outs = pl.pallas_call(
        body,
        grid=(1,),
        in_specs=[whole(pltpu.SMEM)] + [whole()] * 6 + [w_spec, w_spec],
        out_specs=[whole()] * len(shapes),
        out_shape=[jax.ShapeDtypeStruct(sh, BF16) for sh in shapes],
        compiler_params=params(),
        name="project",
    )(places, norm, *rows_of, own, other)
    return outs


def attend(q, own, other, gates, key_place, query_place):
    blocks, rows, _ = q.shape
    span = 8 * rows
    group = 4
    tall = group * rows
    count = blocks // group

    def body(q_ref, *refs):
        kvs, (gate_ref, kp_ref, qp_ref, out_ref, acc_ref, top_ref) = refs[:10], refs[10:]
        ones = jnp.ones((span, HD), BF16)

        def pieces(s, kind, late):
            out = []
            for side in (kvs[:5], kvs[5:]):
                out += [side[0][s, kind], side[1][s, kind], side[2][s, kind]]
                out.append(side[4][s - blocks // 2, kind] if late else side[3][s, kind])
            return jnp.concatenate(out, axis=0)

        def step(s, first_group, fresh, late):
            k = pieces(s, 0, late)
            v = jnp.concatenate([pieces(s, 1, late), ones], axis=1)
            gate = gate_ref[s]
            for g in range(first_group, count):
                at = pl.ds(g * tall, tall)
                qt = q_ref[g * group : (g + 1) * group].reshape(tall, HD)
                sc = lax.dot_general(
                    qt, k, (((1,), (1,)), ((), ())), preferred_element_type=F32
                )
                sc = sc - gate
                if g == first_group:
                    sc = jnp.where(kp_ref[...] + s * span <= qp_ref[at], sc, MASKED)
                new = jnp.max(sc, axis=1, keepdims=True)
                if fresh:
                    p = jnp.exp2(sc - new).astype(BF16)
                    acc_ref[at] = jnp.dot(p, v, preferred_element_type=F32)
                else:
                    top = top_ref[at]
                    new = jnp.maximum(top, new)
                    p = jnp.exp2(sc - new).astype(BF16)
                    acc_ref[at] = acc_ref[at] * jnp.exp2(top - new) + jnp.dot(
                        p, v, preferred_element_type=F32
                    )
                top_ref[at] = new

        step(0, 0, True, False)
        for r in range(count):

            def loop(s, carry, r=r):
                step(s, r, False, 2 * r >= count)
                return carry

            lax.fori_loop(max(1, r * group), (r + 1) * group, loop, 0)
        for g in range(count):
            acc = acc_ref[g * tall : (g + 1) * tall]
            out_ref[g * group : (g + 1) * group] = (
                (acc[:, :HD] / acc[:, HD:]).astype(BF16).reshape(group, rows, HD)
            )

    return pl.pallas_call(
        body,
        in_specs=[whole()] * 14,
        out_specs=whole(),
        out_shape=jax.ShapeDtypeStruct(q.shape, BF16),
        scratch_shapes=[
            pltpu.VMEM((blocks * rows, 2 * HD), F32),
            pltpu.VMEM((blocks * rows, 1), F32),
        ],
        compiler_params=params(),
        name="attend",
    )(q, *own, *other, gates, key_place, query_place)


def pool(first, rows_in, border, mix, scale):
    nx, seqs, two, rows, _ = rows_in.shape
    edge = border.shape[3]

    def body(first_ref, in_ref, edge_ref, mix_ref, scale_ref, out_ref):
        at = first_ref[0] + lax.broadcasted_iota(jnp.int32, (rows, 1), 0) + 1
        for x in range(nx):
            for c in range(two):
                group = 2 * x + c
                width = 2 ** (1 + group % 4)
                inverse = 1.0 / jnp.minimum(at, width).astype(F32)
                parts = []
                for i in range(seqs):
                    own = in_ref[x, i, c].astype(F32)
                    total = jnp.concatenate([edge_ref[x, i, c].astype(F32), own], axis=0)
                    by = 1
                    while by < width:
                        total = total + pltpu.roll(total, by, 0)
                        by *= 2
                    parts.append((total[edge:] * inverse - own).astype(BF16))
                mixed = jnp.dot(
                    jnp.concatenate(parts, axis=0), mix_ref[group], preferred_element_type=F32
                )
                mixed = (mixed * scale_ref[group : group + 1, :]).astype(BF16)
                for i in range(seqs):
                    out_ref[x, i, c] = mixed[i * rows : (i + 1) * rows]

    return pl.pallas_call(
        body,
        in_specs=[whole(pltpu.SMEM)] + [whole()] * 4,
        out_specs=whole(),
        out_shape=jax.ShapeDtypeStruct(rows_in.shape, BF16),
        compiler_params=params(),
        name="pool",
    )(first, rows_in, border, mix, scale)


def finish(places, pooled, attn, own, other):
    nx, seqs, _, rows, _ = pooled.shape
    ny, deep, wide = own[0].shape

    def body(p_ref, pool_ref, attn_ref, *refs):
        out_ref = refs[10]
        late = pl.program_id(0) >= ny // 2
        total = jnp.zeros((seqs * rows, wide), F32)
        for side, c in ((refs[:5], p_ref[0]), (refs[5:10], 1 - p_ref[0])):
            for a in range(nx):
                x = p_ref[1 + a]
                left = jnp.concatenate(
                    [
                        jnp.concatenate([pool_ref[x, i, c] for i in range(seqs)], axis=0),
                        jnp.concatenate([attn_ref[x, i, c] for i in range(seqs)], axis=0),
                    ],
                    axis=1,
                )
                right = side[a][0] if a < 3 else jnp.where(late, side[4][0], side[3][0])
                total = total + jnp.dot(left, right, preferred_element_type=F32)
        out_ref[...] = total.astype(BF16).reshape(seqs, rows, wide)

    half = ny // 2
    shape = (1, deep, wide)
    specs = [pl.BlockSpec(shape, lambda j: (j, 0, 0))] * 3 + [
        pl.BlockSpec(shape, lambda j: (jnp.minimum(j, half - 1), 0, 0)),
        pl.BlockSpec(shape, lambda j: (jnp.maximum(j - half, 0), 0, 0)),
    ]
    return pl.pallas_call(
        body,
        grid=(ny,),
        in_specs=[whole(pltpu.SMEM), whole(), whole()] + specs + specs,
        out_specs=pl.BlockSpec((seqs, rows, wide), lambda j: (0, 0, j)),
        out_shape=jax.ShapeDtypeStruct((seqs, rows, ny * wide), BF16),
        compiler_params=params(),
        name="finish",
    )(places, pooled, attn, *own, *other)


def after(x, *others):
    return lax.optimization_barrier((x,) + others)[0]


def placed(pieces, where, dim):
    shape = list(pieces[0].shape)
    shape[dim] = len(pieces)
    out = jnp.zeros(shape, pieces[0].dtype)
    for piece, at in zip(pieces, where):
        out = lax.dynamic_update_slice_in_dim(out, piece, at, dim)
    return out


def on_device(
    tokens,
    norm_gain,
    w_pool_in,
    pool_mix,
    pool_scale,
    w_query,
    w_key,
    w_value,
    gate_cache,
    w_out_pool,
    w_out_attn,
):
    z = lax.axis_index("sp")
    x = lax.axis_index("tp_0")
    y = lax.axis_index("fs")
    c = lax.axis_index("tp_1")
    planes = lax.axis_size("sp")
    chunks = lax.axis_size("tp_0")
    seqs, rows, depth = tokens.shape
    block = rows * chunks * 2
    seen = [x, (x + 3) % 4, (x + 1) % 4, (x + 2) % 4]
    places = jnp.stack([c] + seen).astype(jnp.int32)

    deep = w_key.shape[0]
    gain = lax.dynamic_slice_in_dim(norm_gain, y * deep, deep, 0)
    all_rows = ring_of_four(tokens, "tp_0")
    norm = factors_of(all_rows)
    weights = jnp.concatenate([w_key, w_value, w_query, w_pool_in], axis=1)
    weights = (weights.astype(F32) * gain[:, None]).astype(BF16)
    own_w = spread(weights, "fs").reshape(depth, -1)
    other_w = sibling(own_w)

    (kv,) = project(places, norm, all_rows, own_w, other_w, 0, (1.0, 1.0), False)
    kv_here = lax.all_to_all(kv, "tp_0", 0, 0, tiled=True)
    kv = lax.all_to_all(
        kv_here.reshape(planes, 2, rows, HD), "sp", 0, 0, tiled=True
    )
    qp = project(
        places, norm, all_rows, own_w, other_w, 1, (HD**-0.5 * LOG2E, 1.0), True
    )
    got = [qp[0]]
    for piece, by in zip(qp[1:], (-1, 1, 2)):
        got.append(
            lax.ppermute(piece, "tp_0", [(i, (i + by) % 4) for i in range(4)])
        )
    came = [x, (x + 1) % 4, (x + 3) % 4, (x + 2) % 4]
    qp = placed(got, came, 1)

    pair_seq = (z // 2) % 2
    pair_head = 2 * (z // 4) + z % 2
    gate_rows = lax.dynamic_index_in_dim(gate_cache[:, 0], pair_seq, 0, keepdims=False)
    gate_all = lax.all_gather(after(gate_rows, kv_here), TP, axis=0, tiled=False)
    gate = lax.dynamic_index_in_dim(gate_all, pair_head, 0, keepdims=False) * LOG2E
    gate = gate.reshape(planes, chunks, 2, rows).transpose(0, 2, 1, 3)
    gate = jnp.where(c == 0, gate, gate[:, ::-1])
    gate = jnp.concatenate([lax.dynamic_slice_in_dim(gate, at, 1, 2) for at in seen], axis=2)
    gate = gate.reshape(planes, 1, block)

    q = after(qp[0].reshape(planes, rows, HD), kv, gate)
    q = lax.all_to_all(q, "sp", 0, 0, tiled=True)
    pool_in = qp[1]
    total = planes * chunks * 2
    border = lax.ppermute(
        pool_in[:, :, :, rows - 16 :], SP_TP, [(i, i + 1) for i in range(total - 1)]
    )
    first = (z * block + (2 * x + c) * rows).reshape(1).astype(jnp.int32)
    pooled = pool(first, pool_in, border, pool_mix, pool_scale.reshape(-1, HD))

    kv_own = ring_of_four(kv, "tp_0")
    kv_other = [sibling(piece) for piece in kv_own]

    out_w = jnp.concatenate([w_out_pool, w_out_attn], axis=0)
    o = ring_of_four(after(out_w, own_w), "fs")
    o = [o[0], o[1], o[2], jnp.concatenate(o[3:], axis=0)]
    o = placed([w[None] for w in o], [y, (y + 3) % 4, (y + 1) % 4, (y + 2) % 4], 0)
    out_own = ring_of_four(after(o, kv_here), "tp_0")
    out_other = [sibling(piece) for piece in out_own]

    at = jnp.arange(rows, dtype=jnp.int32)
    key_place = jnp.concatenate(
        [((2 * s + cc) * rows + at) for cc in (c, 1 - c) for s in seen]
    ).reshape(1, -1).astype(jnp.int32)
    query_place = (
        jnp.arange(planes, dtype=jnp.int32)[:, None] * block + (2 * x + c) * rows + at[None]
    ).reshape(-1, 1)
    attn = attend(q, kv_own, kv_other, gate, key_place, query_place)
    attn = lax.all_to_all(attn, "sp", 0, 0, tiled=True)
    attn = attn.reshape(chunks, seqs, 2, rows, HD)
    return finish(places, pooled, attn, out_own, out_other)


def solution(mesh):
    torus = Mesh(
        mesh.devices.reshape(mesh.shape["sp"], mesh.shape["fs"], 4, 2), ("sp", "fs", "tp_0", "tp_1")
    )
    return jax.shard_map(
        on_device,
        mesh=torus,
        in_specs=(
            P("fs", SP_TP, None),
            P(),
            P("fs", TP),
            P(),
            P(),
            P("fs", TP),
            P("fs", TP),
            P("fs", TP),
            P("fs", TP, None),
            P(TP, "fs"),
            P(TP, "fs"),
        ),
        out_specs=P("fs", SP_TP, None),
        check_vma=False,
    )
```

```python
import jax
import jax.numpy as jnp
from jax import lax
from jax.experimental import pallas as pl
from jax.experimental.pallas import tpu as pltpu
from jax.sharding import Mesh
from jax.sharding import PartitionSpec as P

HD = 128
TP = ("tp_0", "tp_1")
SP_TP = ("sp", "tp_0", "tp_1")
EPS = 1e-06
MASKED = -1e30
GATE_ROWS = 16
LOG2E = 1.4426950408889634
F32 = jnp.float32
BF16 = jnp.bfloat16
VMEM_LIMIT = 56 * 1024 * 1024


def params(**kw):
    return pltpu.CompilerParams(vmem_limit_bytes=VMEM_LIMIT, **kw)


def whole(memory=pltpu.VMEM):
    return pl.BlockSpec(memory_space=memory)


def spread(x, axis):
    n = lax.axis_size(axis)
    return lax.all_to_all(jnp.broadcast_to(x[None], (n,) + x.shape), axis, 0, 0, tiled=True)


def sibling(x):
    return lax.ppermute(x, "tp_1", [(0, 1), (1, 0)])


UP = [(i, (i + 1) % 4) for i in range(4)]
DOWN = [(i, (i - 1) % 4) for i in range(4)]


def hops(x, axis):
    return lax.ppermute(x, axis, UP), lax.ppermute(x, axis, DOWN)


def relays(before, after, axis):
    half = before.shape[0] // 2
    return lax.ppermute(before[:half], axis, UP), lax.ppermute(after[half:], axis, DOWN)


def ring_of_four(x, axis):
    near = hops(x, axis)
    return (x, *near, *relays(*near, axis))


def rms(x):
    wide = x.astype(F32)
    return lax.rsqrt(jnp.mean(wide * wide, axis=-1, keepdims=True) + EPS)


def factors_of(rows_of):
    seqs, rows, _ = rows_of[0].shape

    def body(x0, x1, x2, x3, x4, out_ref):
        at = 0
        for ref in (x0, x1, x2, x3, x4):
            for i in range(ref.shape[0]):
                out_ref[at : at + rows] = rms(ref[i])
                at += rows

    return pl.pallas_call(
        body,
        in_specs=[whole()] * 5,
        out_specs=whole(),
        out_shape=jax.ShapeDtypeStruct((4 * seqs * rows, 1), F32),
        compiler_params=params(),
        name="factors",
    )(*rows_of)


def project(places, norm, rows_of, own, other, half, factors, split):
    seqs, rows, _ = rows_of[0].shape
    kinds = len(factors)

    def body(p_ref, norm_ref, x0, x1, x2, x3, x4, own_ref, other_ref, *outs):
        x = jnp.concatenate(
            [x0[0], x0[1], x1[0], x1[1], x2[0], x2[1], x3[0], x4[0]], axis=0
        )
        r = norm_ref[...]
        lane = lax.broadcasted_iota(jnp.int32, (GATE_ROWS, HD), 1)
        first_half = (lane < rows) == (p_ref[0] == 0)
        for ref, head in ((own_ref, p_ref[0]), (other_ref, 1 - p_ref[0])):
            w = jnp.concatenate(
                [ref[b, : ref.shape[1] - GATE_ROWS, cols] for b in range(ref.shape[0])], axis=0
            )
            y = jnp.dot(x, w, preferred_element_type=F32) * r
            if not split:
                for a in range(4):
                    to = p_ref[1 + a]
                    g = ref[
                        p_ref[5],
                        ref.shape[1] - GATE_ROWS :,
                        pl.ds(pl.multiple_of(to * 2 * rows, 2 * rows), 2 * rows),
                    ].astype(F32)
                    turned = pltpu.roll(g, rows, 1)
                    twice = jnp.where(first_half, g, turned).astype(BF16)
                    for i in range(seqs):
                        outs[0][to, i, head, 2 * rows :] = (
                            twice if i == 0 else jnp.roll(twice, -i * 8, 0)
                        )
            for kind, factor in enumerate(factors):
                part = y[:, kind * HD : (kind + 1) * HD]
                if factor != 1.0:
                    part = part * factor
                part = part.astype(BF16)
                for a in range(4):
                    for i in range(seqs):
                        at = (a * seqs + i) * rows
                        if split:
                            outs[a][kind, 0, i, head] = part[at : at + rows]
                        else:
                            outs[0][p_ref[1 + a], i, head, kind * rows : (kind + 1) * rows] = part[
                                at : at + rows
                            ]

    cols = slice(half * kinds * HD, (half + 1) * kinds * HD)
    if split:
        shapes = [(kinds, 1, seqs, 2, rows, HD)] * 4
    else:
        shapes = [(4, seqs, 2, kinds * rows + GATE_ROWS, HD)]
    outs = pl.pallas_call(
        body,
        in_specs=[whole(pltpu.SMEM)] + [whole()] * 8,
        out_specs=[whole()] * len(shapes),
        out_shape=[jax.ShapeDtypeStruct(sh, BF16) for sh in shapes],
        compiler_params=params(),
        name="project",
    )(places, norm, *rows_of, own, other)
    return outs


def attend(q, own, other, key_place, query_place):
    blocks, rows, _ = q.shape
    span = 8 * rows
    group = 4
    tall = group * rows
    count = blocks // group

    def body(q_ref, *refs):
        kvs, (kp_ref, qp_ref, out_ref, acc_ref, top_ref) = refs[:7], refs[7:]
        ones = jnp.ones((span, HD), BF16)
        left = lax.broadcasted_iota(jnp.int32, (1, HD), 1) < rows

        def blocks_of(s, late, at):
            far = kvs[4][s - blocks // 2, at] if late else kvs[3][s, at]
            return [kvs[0][s, at], kvs[1][s, at], kvs[2][s, at], far, kvs[5][s, at]] + [
                kvs[6][s + n * blocks, at] for n in range(3)
            ]

        def gates(s, late):
            parts = blocks_of(s, late, slice(2 * rows, 2 * rows + GATE_ROWS))
            parts = [jnp.sum(part.astype(F32)[:3], axis=0, keepdims=True) for part in parts]
            return LOG2E * jnp.concatenate(
                [jnp.where(left, parts[n], parts[n + 1]) for n in range(0, 8, 2)], axis=1
            )

        def step(s, first_group, fresh, late):
            k = jnp.concatenate(blocks_of(s, late, slice(0, rows)), axis=0)
            v = jnp.concatenate(blocks_of(s, late, slice(rows, 2 * rows)), axis=0)
            v = jnp.concatenate([v, ones], axis=1)
            gate = gates(s, late)
            for g in range(first_group, count):
                at = pl.ds(g * tall, tall)
                qt = q_ref[g * group : (g + 1) * group].reshape(tall, HD)
                sc = lax.dot_general(
                    qt, k, (((1,), (1,)), ((), ())), preferred_element_type=F32
                )
                sc = sc - gate
                if g == first_group:
                    sc = jnp.where(kp_ref[...] + s * span <= qp_ref[at], sc, MASKED)
                new = jnp.max(sc, axis=1, keepdims=True)
                if fresh:
                    p = jnp.exp2(sc - new).astype(BF16)
                    acc_ref[at] = jnp.dot(p, v, preferred_element_type=F32)
                else:
                    top = top_ref[at]
                    new = jnp.maximum(top, new)
                    p = jnp.exp2(sc - new).astype(BF16)
                    acc_ref[at] = acc_ref[at] * jnp.exp2(top - new) + jnp.dot(
                        p, v, preferred_element_type=F32
                    )
                top_ref[at] = new

        step(0, 0, True, False)
        for r in range(count):

            def loop(s, carry, r=r):
                step(s, r, False, 2 * r >= count)
                return carry

            lax.fori_loop(max(1, r * group), (r + 1) * group, loop, 0)
        for g in range(count):
            acc = acc_ref[g * tall : (g + 1) * tall]
            out_ref[g * group : (g + 1) * group] = (
                (acc[:, :HD] / acc[:, HD:]).astype(BF16).reshape(group, rows, HD)
            )

    return pl.pallas_call(
        body,
        in_specs=[whole()] * 10,
        out_specs=whole(),
        out_shape=jax.ShapeDtypeStruct(q.shape, BF16),
        scratch_shapes=[
            pltpu.VMEM((blocks * rows, 2 * HD), F32),
            pltpu.VMEM((blocks * rows, 1), F32),
        ],
        compiler_params=params(),
        name="attend",
    )(q, *own, *other, key_place, query_place)


def pool(first, rows_in, border, mix, scale):
    nx, seqs, two, rows, _ = rows_in.shape
    edge = border.shape[3]

    def body(first_ref, in_ref, edge_ref, mix_ref, scale_ref, out_ref):
        at = first_ref[0] + lax.broadcasted_iota(jnp.int32, (rows, 1), 0) + 1
        for x in range(nx):
            for c in range(two):
                group = 2 * x + c
                width = 2 ** (1 + group % 4)
                inverse = 1.0 / jnp.minimum(at, width).astype(F32)
                parts = []
                for i in range(seqs):
                    own = in_ref[x, i, c].astype(F32)
                    total = jnp.concatenate([edge_ref[x, i, c].astype(F32), own], axis=0)
                    by = 1
                    while by < width:
                        total = total + pltpu.roll(total, by, 0)
                        by *= 2
                    parts.append((total[edge:] * inverse - own).astype(BF16))
                mixed = jnp.dot(
                    jnp.concatenate(parts, axis=0), mix_ref[group], preferred_element_type=F32
                )
                mixed = (mixed * scale_ref[group : group + 1, :]).astype(BF16)
                for i in range(seqs):
                    out_ref[x, i, c] = mixed[i * rows : (i + 1) * rows]

    return pl.pallas_call(
        body,
        in_specs=[whole(pltpu.SMEM)] + [whole()] * 4,
        out_specs=whole(),
        out_shape=jax.ShapeDtypeStruct(rows_in.shape, BF16),
        compiler_params=params(),
        name="pool",
    )(first, rows_in, border, mix, scale)


def finish(places, pooled, attn, own, other):
    nx, seqs, _, rows, _ = pooled.shape
    ny, deep, wide = own[0].shape

    def body(p_ref, pool_ref, attn_ref, *refs):
        out_ref = refs[10]
        late = pl.program_id(0) >= ny // 2
        total = jnp.zeros((seqs * rows, wide), F32)
        for side, c in ((refs[:5], p_ref[0]), (refs[5:10], 1 - p_ref[0])):
            for a in range(nx):
                x = p_ref[1 + a]
                left = jnp.concatenate(
                    [
                        jnp.concatenate([pool_ref[x, i, c] for i in range(seqs)], axis=0),
                        jnp.concatenate([attn_ref[x, i, c] for i in range(seqs)], axis=0),
                    ],
                    axis=1,
                )
                right = side[a][0] if a < 3 else jnp.where(late, side[4][0], side[3][0])
                total = total + jnp.dot(left, right, preferred_element_type=F32)
        out_ref[...] = total.astype(BF16).reshape(seqs, rows, wide)

    half = ny // 2
    shape = (1, deep, wide)
    specs = [pl.BlockSpec(shape, lambda j: (j, 0, 0))] * 3 + [
        pl.BlockSpec(shape, lambda j: (jnp.minimum(j, half - 1), 0, 0)),
        pl.BlockSpec(shape, lambda j: (jnp.maximum(j - half, 0), 0, 0)),
    ]
    return pl.pallas_call(
        body,
        grid=(ny,),
        in_specs=[whole(pltpu.SMEM), whole(), whole()] + specs + specs,
        out_specs=pl.BlockSpec((seqs, rows, wide), lambda j: (0, 0, j)),
        out_shape=jax.ShapeDtypeStruct((seqs, rows, ny * wide), BF16),
        compiler_params=params(),
        name="finish",
    )(places, pooled, attn, *own, *other)


def after(x, *others):
    return lax.optimization_barrier((x,) + others)[0]


def placed(pieces, where, dim):
    shape = list(pieces[0].shape)
    shape[dim] = len(pieces)
    out = jnp.zeros(shape, pieces[0].dtype)
    for piece, at in zip(pieces, where):
        out = lax.dynamic_update_slice_in_dim(out, piece, at, dim)
    return out


def on_device(
    tokens,
    norm_gain,
    w_pool_in,
    pool_mix,
    pool_scale,
    w_query,
    w_key,
    w_value,
    gate_cache,
    w_out_pool,
    w_out_attn,
):
    z = lax.axis_index("sp")
    x = lax.axis_index("tp_0")
    y = lax.axis_index("fs")
    c = lax.axis_index("tp_1")
    planes = lax.axis_size("sp")
    chunks = lax.axis_size("tp_0")
    seqs, rows, _ = tokens.shape
    block = rows * chunks * 2
    seen = [x, (x + 3) % 4, (x + 1) % 4, (x + 2) % 4]
    places = jnp.stack([c] + seen + [y]).astype(jnp.int32)

    deep = w_key.shape[0]
    gain = lax.dynamic_slice_in_dim(norm_gain, y * deep, deep, 0)
    all_rows = ring_of_four(tokens, "tp_0")
    norm = factors_of(all_rows)
    weights = jnp.concatenate([w_key, w_value, w_query, w_pool_in], axis=1)
    weights = (weights.astype(F32) * gain[:, None]).astype(BF16)
    here = lax.dynamic_slice_in_dim(gate_cache[:, 0], z * block, block, 1)
    high = lax.reduce_precision(here, 8, 7)
    rest = here - high
    middle = lax.reduce_precision(rest, 8, 7)
    parts = jnp.stack([high, middle, rest - middle], axis=1).astype(BF16)
    parts = jnp.pad(parts, ((0, 0), (0, 5), (0, 0))).reshape(GATE_ROWS, block)
    own_w = spread(jnp.concatenate([weights, parts], axis=0), "fs")
    other_w = sibling(own_w)

    (kv,) = project(places, norm, all_rows, own_w, other_w, 0, (1.0, 1.0), False)
    kv_here = lax.all_to_all(kv, "tp_0", 0, 0, tiled=True)
    kv = lax.all_to_all(kv_here.reshape(planes, 2 * rows + GATE_ROWS, HD), "sp", 0, 0, tiled=True)
    qp = project(
        places, norm, all_rows, own_w, other_w, 1, (HD**-0.5 * LOG2E, 1.0), True
    )
    got = [qp[0]]
    for piece, by in zip(qp[1:], (-1, 1, 2)):
        got.append(
            lax.ppermute(piece, "tp_0", [(i, (i + by) % 4) for i in range(4)])
        )
    came = [x, (x + 1) % 4, (x + 3) % 4, (x + 2) % 4]
    qp = placed(got, came, 1)

    q = after(qp[0].reshape(planes, rows, HD), kv)
    q = lax.all_to_all(q, "sp", 0, 0, tiled=True)
    pool_in = qp[1]
    total = planes * chunks * 2
    border = lax.ppermute(
        pool_in[:, :, :, rows - 16 :], SP_TP, [(i, i + 1) for i in range(total - 1)]
    )
    first = (z * block + (2 * x + c) * rows).reshape(1).astype(jnp.int32)
    pooled = pool(first, pool_in, border, pool_mix, pool_scale.reshape(-1, HD))

    kv_own = ring_of_four(kv, "tp_0")
    kv_other = [sibling(kv), sibling(jnp.concatenate(kv_own[1:], axis=0))]

    out_w = jnp.concatenate([w_out_pool, w_out_attn], axis=0)
    o = ring_of_four(after(out_w, own_w), "fs")
    o = [o[0], o[1], o[2], jnp.concatenate(o[3:], axis=0)]
    o = placed([w[None] for w in o], [y, (y + 3) % 4, (y + 1) % 4, (y + 2) % 4], 0)
    out_near = hops(after(o, kv_here), "tp_0")

    at = jnp.arange(rows, dtype=jnp.int32)
    key_place = jnp.concatenate(
        [((2 * s + cc) * rows + at) for cc in (c, 1 - c) for s in seen]
    ).reshape(1, -1).astype(jnp.int32)
    query_place = (
        jnp.arange(planes, dtype=jnp.int32)[:, None] * block + (2 * x + c) * rows + at[None]
    ).reshape(-1, 1)
    attn = attend(q, kv_own, kv_other, key_place, query_place)
    out_near = lax.optimization_barrier((*out_near, attn))[:2]
    out_own = (o, *out_near, *relays(*out_near, "tp_0"))
    out_other = [sibling(piece) for piece in (after(o, attn), *out_own[1:])]
    attn = lax.all_to_all(attn, "sp", 0, 0, tiled=True)
    attn = attn.reshape(chunks, seqs, 2, rows, HD)
    return finish(places, pooled, attn, out_own, out_other)


def solution(mesh):
    torus = Mesh(
        mesh.devices.reshape(mesh.shape["sp"], mesh.shape["fs"], 4, 2), ("sp", "fs", "tp_0", "tp_1")
    )
    return jax.shard_map(
        on_device,
        mesh=torus,
        in_specs=(
            P("fs", SP_TP, None),
            P(),
            P("fs", TP),
            P(),
            P(),
            P("fs", TP),
            P("fs", TP),
            P("fs", TP),
            P("fs", TP, None),
            P(TP, "fs"),
            P(TP, "fs"),
        ),
        out_specs=P("fs", SP_TP, None),
        check_vma=False,
    )
```

```python
import jax
import jax.numpy as jnp
from jax import lax
from jax.experimental import pallas as pl
from jax.experimental.pallas import tpu as pltpu
from jax.sharding import Mesh
from jax.sharding import PartitionSpec as P

HD = 128
TP = ("tp_0", "tp_1")
SP_TP = ("sp", "tp_0", "tp_1")
EPS = 1e-06
MASKED = -1e30
GATE_ROWS = 16
LOG2E = 1.4426950408889634
F32 = jnp.float32
BF16 = jnp.bfloat16
VMEM_LIMIT = 56 * 1024 * 1024


def params(**kw):
    return pltpu.CompilerParams(vmem_limit_bytes=VMEM_LIMIT, **kw)


def whole(memory=pltpu.VMEM):
    return pl.BlockSpec(memory_space=memory)


def sibling(x):
    return lax.ppermute(x, "tp_1", [(0, 1), (1, 0)])


UP = [(i, (i + 1) % 4) for i in range(4)]
DOWN = [(i, (i - 1) % 4) for i in range(4)]


def hops(x, axis):
    return lax.ppermute(x, axis, UP), lax.ppermute(x, axis, DOWN)


def relays(before, after, axis):
    half = before.shape[0] // 2
    return lax.ppermute(before[:half], axis, UP), lax.ppermute(after[half:], axis, DOWN)


def ring_of_four(x, axis):
    near = hops(x, axis)
    return (x, *near, *relays(*near, axis))


def rms(x):
    wide = x.astype(F32)
    return lax.rsqrt(jnp.mean(wide * wide, axis=-1, keepdims=True) + EPS)


def factors_of(rows_of):
    seqs, rows, _ = rows_of[0].shape

    def body(x0, x1, x2, x3, x4, out_ref):
        at = 0
        for ref in (x0, x1, x2, x3, x4):
            for i in range(ref.shape[0]):
                out_ref[at : at + rows] = rms(ref[i])
                at += rows

    return pl.pallas_call(
        body,
        in_specs=[whole()] * 5,
        out_specs=whole(),
        out_shape=jax.ShapeDtypeStruct((4 * seqs * rows, 1), F32),
        compiler_params=params(),
        name="factors",
    )(*rows_of)


def project(places, norm, rows_of, own, other, half, factors, split):
    seqs, rows, _ = rows_of[0].shape
    kinds = len(factors)

    def body(p_ref, norm_ref, *refs):
        xs, own_refs, other_refs, outs = refs[:5], refs[5:10], refs[10:12], refs[12:]
        deep = own_refs[0].shape[0] - GATE_ROWS
        tall = deep + GATE_ROWS
        r = norm_ref[...]
        lane = lax.broadcasted_iota(jnp.int32, (GATE_ROWS, HD), 1)
        first_half = (lane < rows) == (p_ref[0] == 0)
        slabs = []
        for b in range(4):
            at = pl.ds(pl.multiple_of(p_ref[5 + b] * deep, deep), deep)
            slabs.append(
                jnp.concatenate(
                    [ref[i, :, at] for ref in xs for i in range(ref.shape[0])], axis=0
                )
            )
        own = [ref[:deep, cols] for ref in own_refs[:3]]
        far = jnp.concatenate([ref[:, cols] for ref in own_refs[3:]], axis=0)
        own.append(far[:deep])
        other = [other_refs[0][:deep, cols]]
        other += [other_refs[1][n * tall : n * tall + deep, cols] for n in range(3)]
        for ref, ws, head in (
            (own_refs[0], own, p_ref[0]),
            (other_refs[0], other, 1 - p_ref[0]),
        ):
            y = jnp.dot(slabs[0], ws[0], preferred_element_type=F32)
            for b in range(1, 4):
                y = y + jnp.dot(slabs[b], ws[b], preferred_element_type=F32)
            y = y * r
            if not split:
                for a in range(4):
                    to = p_ref[1 + a]
                    g = ref[
                        deep:,
                        pl.ds(pl.multiple_of(to * 2 * rows, 2 * rows), 2 * rows),
                    ].astype(F32)
                    turned = pltpu.roll(g, rows, 1)
                    twice = jnp.where(first_half, g, turned).astype(BF16)
                    for i in range(seqs):
                        outs[0][to, i, head, 2 * rows :] = (
                            twice if i == 0 else jnp.roll(twice, -i * 8, 0)
                        )
            for kind, factor in enumerate(factors):
                part = y[:, kind * HD : (kind + 1) * HD]
                if factor != 1.0:
                    part = part * factor
                part = part.astype(BF16)
                for a in range(4):
                    for i in range(seqs):
                        at = (a * seqs + i) * rows
                        if split:
                            outs[a][kind, 0, i, head] = part[at : at + rows]
                        else:
                            outs[0][p_ref[1 + a], i, head, kind * rows : (kind + 1) * rows] = part[
                                at : at + rows
                            ]

    cols = slice(half * kinds * HD, (half + 1) * kinds * HD)
    if split:
        shapes = [(kinds, 1, seqs, 2, rows, HD)] * 4
    else:
        shapes = [(4, seqs, 2, kinds * rows + GATE_ROWS, HD)]
    outs = pl.pallas_call(
        body,
        in_specs=[whole(pltpu.SMEM)] + [whole()] * 13,
        out_specs=[whole()] * len(shapes),
        out_shape=[jax.ShapeDtypeStruct(sh, BF16) for sh in shapes],
        compiler_params=params(),
        name="project",
    )(places, norm, *rows_of, *own, *other)
    return outs


def attend(q, own, other, key_place, query_place):
    blocks, rows, _ = q.shape
    span = 8 * rows
    group = 4
    tall = group * rows
    count = blocks // group

    def body(q_ref, *refs):
        kvs, (kp_ref, qp_ref, out_ref, acc_ref, top_ref) = refs[:7], refs[7:]
        ones = jnp.ones((span, HD), BF16)
        left = lax.broadcasted_iota(jnp.int32, (1, HD), 1) < rows

        def blocks_of(s, late, at):
            far = kvs[4][s - blocks // 2, at] if late else kvs[3][s, at]
            return [kvs[0][s, at], kvs[1][s, at], kvs[2][s, at], far, kvs[5][s, at]] + [
                kvs[6][s + n * blocks, at] for n in range(3)
            ]

        def gates(s, late):
            parts = blocks_of(s, late, slice(2 * rows, 2 * rows + GATE_ROWS))
            parts = [jnp.sum(part.astype(F32)[:3], axis=0, keepdims=True) for part in parts]
            return LOG2E * jnp.concatenate(
                [jnp.where(left, parts[n], parts[n + 1]) for n in range(0, 8, 2)], axis=1
            )

        def step(s, first_group, fresh, late):
            k = jnp.concatenate(blocks_of(s, late, slice(0, rows)), axis=0)
            v = jnp.concatenate(blocks_of(s, late, slice(rows, 2 * rows)), axis=0)
            v = jnp.concatenate([v, ones], axis=1)
            gate = gates(s, late)
            for g in range(first_group, count):
                at = pl.ds(g * tall, tall)
                qt = q_ref[g * group : (g + 1) * group].reshape(tall, HD)
                sc = lax.dot_general(
                    qt, k, (((1,), (1,)), ((), ())), preferred_element_type=F32
                )
                sc = sc - gate
                if g == first_group:
                    sc = jnp.where(kp_ref[...] + s * span <= qp_ref[at], sc, MASKED)
                new = jnp.max(sc, axis=1, keepdims=True)
                if fresh:
                    p = jnp.exp2(sc - new).astype(BF16)
                    acc_ref[at] = jnp.dot(p, v, preferred_element_type=F32)
                else:
                    top = top_ref[at]
                    new = jnp.maximum(top, new)
                    p = jnp.exp2(sc - new).astype(BF16)
                    acc_ref[at] = acc_ref[at] * jnp.exp2(top - new) + jnp.dot(
                        p, v, preferred_element_type=F32
                    )
                top_ref[at] = new

        step(0, 0, True, False)
        for r in range(count):

            def loop(s, carry, r=r):
                step(s, r, False, 2 * r >= count)
                return carry

            lax.fori_loop(max(1, r * group), (r + 1) * group, loop, 0)
        for g in range(count):
            acc = acc_ref[g * tall : (g + 1) * tall]
            out_ref[g * group : (g + 1) * group] = (
                (acc[:, :HD] / acc[:, HD:]).astype(BF16).reshape(group, rows, HD)
            )

    return pl.pallas_call(
        body,
        in_specs=[whole()] * 10,
        out_specs=whole(),
        out_shape=jax.ShapeDtypeStruct(q.shape, BF16),
        scratch_shapes=[
            pltpu.VMEM((blocks * rows, 2 * HD), F32),
            pltpu.VMEM((blocks * rows, 1), F32),
        ],
        compiler_params=params(),
        name="attend",
    )(q, *own, *other, key_place, query_place)


def pool(first, rows_in, border, mix, scale):
    nx, seqs, two, rows, _ = rows_in.shape
    edge = border.shape[3]

    def body(first_ref, in_ref, edge_ref, mix_ref, scale_ref, out_ref):
        at = first_ref[0] + lax.broadcasted_iota(jnp.int32, (rows, 1), 0) + 1
        for x in range(nx):
            for c in range(two):
                group = 2 * x + c
                width = 2 ** (1 + group % 4)
                inverse = 1.0 / jnp.minimum(at, width).astype(F32)
                parts = []
                for i in range(seqs):
                    own = in_ref[x, i, c].astype(F32)
                    total = jnp.concatenate([edge_ref[x, i, c].astype(F32), own], axis=0)
                    by = 1
                    while by < width:
                        total = total + pltpu.roll(total, by, 0)
                        by *= 2
                    parts.append((total[edge:] * inverse - own).astype(BF16))
                mixed = jnp.dot(
                    jnp.concatenate(parts, axis=0), mix_ref[group], preferred_element_type=F32
                )
                mixed = (mixed * scale_ref[group : group + 1, :]).astype(BF16)
                for i in range(seqs):
                    out_ref[x, i, c] = mixed[i * rows : (i + 1) * rows]

    return pl.pallas_call(
        body,
        in_specs=[whole(pltpu.SMEM)] + [whole()] * 4,
        out_specs=whole(),
        out_shape=jax.ShapeDtypeStruct(rows_in.shape, BF16),
        compiler_params=params(),
        name="pool",
    )(first, rows_in, border, mix, scale)


def finish(places, pooled, attn, pooled_pair, attn_pair, w):
    nx, seqs, _, rows, _ = pooled.shape
    ny, deep, wide = w[0].shape
    own = seqs * rows

    def body(p_ref, pool_ref, attn_ref, pool_pair_ref, attn_pair_ref, *refs):
        out_ref, pair_ref = refs[5:]
        late = pl.program_id(0) >= ny // 2
        c = p_ref[0]
        total = jnp.zeros((2 * own, wide), F32)
        for a in range(nx):
            x = p_ref[1 + a]
            left = jnp.concatenate(
                [
                    jnp.concatenate(
                        [ref[x, i, c] for ref in two for i in range(seqs)], axis=0
                    )
                    for two in ((pool_ref, pool_pair_ref), (attn_ref, attn_pair_ref))
                ],
                axis=1,
            )
            right = refs[a][0] if a < 3 else jnp.where(late, refs[4][0], refs[3][0])
            total = total + jnp.dot(left, right, preferred_element_type=F32)
        out_ref[...] = total[:own].reshape(seqs, rows, wide)
        pair_ref[...] = total[own:].astype(BF16).reshape(seqs, rows, wide)

    half = ny // 2
    shape = (1, deep, wide)
    specs = [pl.BlockSpec(shape, lambda j: (j, 0, 0))] * 3 + [
        pl.BlockSpec(shape, lambda j: (jnp.minimum(j, half - 1), 0, 0)),
        pl.BlockSpec(shape, lambda j: (jnp.maximum(j - half, 0), 0, 0)),
    ]
    out_spec = pl.BlockSpec((seqs, rows, wide), lambda j: (0, 0, j))
    out = (seqs, rows, ny * wide)
    return pl.pallas_call(
        body,
        grid=(ny,),
        in_specs=[whole(pltpu.SMEM)] + [whole()] * 4 + specs,
        out_specs=[out_spec, out_spec],
        out_shape=[jax.ShapeDtypeStruct(out, F32), jax.ShapeDtypeStruct(out, BF16)],
        compiler_params=params(),
        name="finish",
    )(places, pooled, attn, pooled_pair, attn_pair, *w)


def after(x, *others):
    return lax.optimization_barrier((x,) + others)[0]


def placed(pieces, where, dim):
    shape = list(pieces[0].shape)
    shape[dim] = len(pieces)
    out = jnp.zeros(shape, pieces[0].dtype)
    for piece, at in zip(pieces, where):
        out = lax.dynamic_update_slice_in_dim(out, piece, at, dim)
    return out


def on_device(
    tokens,
    norm_gain,
    w_pool_in,
    pool_mix,
    pool_scale,
    w_query,
    w_key,
    w_value,
    gate_cache,
    w_out_pool,
    w_out_attn,
):
    z = lax.axis_index("sp")
    x = lax.axis_index("tp_0")
    y = lax.axis_index("fs")
    c = lax.axis_index("tp_1")
    planes = lax.axis_size("sp")
    chunks = lax.axis_size("tp_0")
    seqs, rows, _ = tokens.shape
    block = rows * chunks * 2
    seen = [x, (x + 3) % 4, (x + 1) % 4, (x + 2) % 4]
    deeps = [y, (y + 3) % 4, (y + 1) % 4, (y + 2) % 4]
    places = jnp.stack([c] + seen + deeps).astype(jnp.int32)

    deep = w_key.shape[0]
    gain = lax.dynamic_slice_in_dim(norm_gain, y * deep, deep, 0)
    all_rows = ring_of_four(tokens, "tp_0")
    norm = factors_of(all_rows)
    weights = jnp.concatenate([w_key, w_value, w_query, w_pool_in], axis=1)
    weights = (weights.astype(F32) * gain[:, None]).astype(BF16)
    here = lax.dynamic_slice_in_dim(gate_cache[:, 0], z * block, block, 1)
    high = lax.reduce_precision(here, 8, 7)
    rest = here - high
    middle = lax.reduce_precision(rest, 8, 7)
    parts = jnp.stack([high, middle, rest - middle], axis=1).astype(BF16)
    parts = jnp.pad(parts, ((0, 0), (0, 5), (0, 0))).reshape(GATE_ROWS, block)
    own_w = ring_of_four(jnp.concatenate([weights, parts], axis=0), "fs")
    other_w = sibling(own_w[0])
    other_w = (other_w, sibling(jnp.concatenate(own_w[1:], axis=0)))

    (kv,) = project(places, norm, all_rows, own_w, other_w, 0, (1.0, 1.0), False)
    kv_here = lax.all_to_all(kv, "tp_0", 0, 0, tiled=True)
    kv = lax.all_to_all(kv_here.reshape(planes, 2 * rows + GATE_ROWS, HD), "sp", 0, 0, tiled=True)
    qp = project(
        places, norm, all_rows, own_w, other_w, 1, (HD**-0.5 * LOG2E, 1.0), True
    )
    got = [qp[0]]
    for piece, by in zip(qp[1:], (-1, 1, 2)):
        got.append(
            lax.ppermute(piece, "tp_0", [(i, (i + by) % 4) for i in range(4)])
        )
    came = [x, (x + 1) % 4, (x + 3) % 4, (x + 2) % 4]
    qp = placed(got, came, 1)

    q = after(qp[0].reshape(planes, rows, HD), kv)
    q = lax.all_to_all(q, "sp", 0, 0, tiled=True)
    pool_in = qp[1]
    total = planes * chunks * 2
    border = lax.ppermute(
        pool_in[:, :, :, rows - 16 :], SP_TP, [(i, i + 1) for i in range(total - 1)]
    )
    first = (z * block + (2 * x + c) * rows).reshape(1).astype(jnp.int32)
    pooled = pool(first, pool_in, border, pool_mix, pool_scale.reshape(-1, HD))
    pooled_pair = sibling(pooled)

    kv_own = ring_of_four(kv, "tp_0")
    kv_other = sibling(kv)
    kv_other = (kv_other, sibling(jnp.concatenate(kv_own[1:], axis=0)))

    out_w = jnp.concatenate([w_out_pool, w_out_attn], axis=0)
    o = ring_of_four(after(out_w, own_w[1]), "fs")
    o = [o[0], o[1], o[2], jnp.concatenate(o[3:], axis=0)]
    o = placed([w[None] for w in o], deeps, 0)
    out_near = hops(after(o, kv_here), "tp_0")

    at = jnp.arange(rows, dtype=jnp.int32)
    key_place = jnp.concatenate(
        [((2 * s + cc) * rows + at) for cc in (c, 1 - c) for s in seen]
    ).reshape(1, -1).astype(jnp.int32)
    query_place = (
        jnp.arange(planes, dtype=jnp.int32)[:, None] * block + (2 * x + c) * rows + at[None]
    ).reshape(-1, 1)
    attn = attend(q, kv_own, kv_other, key_place, query_place)
    out_near = lax.optimization_barrier((*out_near, attn))[:2]
    out_own = (o, *out_near, *relays(*out_near, "tp_0"))
    attn = lax.all_to_all(attn, "sp", 0, 0, tiled=True)
    attn = attn.reshape(chunks, seqs, 2, rows, HD)
    mine, theirs = finish(
        places, pooled, attn, pooled_pair, sibling(attn), out_own
    )
    return (mine + sibling(theirs).astype(F32)).astype(BF16)


def solution(mesh):
    torus = Mesh(
        mesh.devices.reshape(mesh.shape["sp"], mesh.shape["fs"], 4, 2), ("sp", "fs", "tp_0", "tp_1")
    )
    return jax.shard_map(
        on_device,
        mesh=torus,
        in_specs=(
            P("fs", SP_TP, None),
            P(),
            P("fs", TP),
            P(),
            P(),
            P("fs", TP),
            P("fs", TP),
            P("fs", TP),
            P("fs", TP, None),
            P(TP, "fs"),
            P(TP, "fs"),
        ),
        out_specs=P("fs", SP_TP, None),
        check_vma=False,
    )
```

```python
import jax
import jax.numpy as jnp
from jax import lax
from jax.experimental import pallas as pl
from jax.experimental.pallas import tpu as pltpu
from jax.sharding import Mesh
from jax.sharding import PartitionSpec as P

HD = 128
TP = ("tp_0", "tp_1")
SP_TP = ("sp", "tp_0", "tp_1")
EPS = 1e-06
MASKED = -1e30
GATE_ROWS = 16
WIDE = 4
LOG2E = 1.4426950408889634
F32 = jnp.float32
BF16 = jnp.bfloat16
VMEM_LIMIT = 56 * 1024 * 1024


def params(**kw):
    return pltpu.CompilerParams(vmem_limit_bytes=VMEM_LIMIT, **kw)


def whole(memory=pltpu.VMEM):
    return pl.BlockSpec(memory_space=memory)


def sibling(x):
    return lax.ppermute(x, "tp_1", [(0, 1), (1, 0)])


UP = [(i, (i + 1) % 4) for i in range(4)]
DOWN = [(i, (i - 1) % 4) for i in range(4)]


def hops(x, axis):
    return lax.ppermute(x, axis, UP), lax.ppermute(x, axis, DOWN)


def relays(before, after, axis):
    half = before.shape[0] // 2
    return lax.ppermute(before[:half], axis, UP), lax.ppermute(after[half:], axis, DOWN)


def ring_of_four(x, axis):
    near = hops(x, axis)
    return (x, *near, *relays(*near, axis))


def ring_in_three(x, axis):
    near = hops(x, axis)
    return (x, *near, lax.ppermute(near[0], axis, UP))


def rms(x):
    wide = x.astype(F32)
    return lax.rsqrt(jnp.mean(wide * wide, axis=-1, keepdims=True) + EPS)


def factors_of(rows_of):
    seqs, rows, _ = rows_of[0].shape

    def body(x0, x1, x2, x3, out_ref):
        at = 0
        for ref in (x0, x1, x2, x3):
            for i in range(ref.shape[0]):
                out_ref[at : at + rows] = rms(ref[i])
                at += rows

    return pl.pallas_call(
        body,
        in_specs=[whole()] * 4,
        out_specs=whole(),
        out_shape=jax.ShapeDtypeStruct((4 * seqs * rows, 1), F32),
        compiler_params=params(),
        name="factors",
    )(*rows_of)


def project(places, norm, rows_of, own, other, half, factors, split):
    seqs, rows, _ = rows_of[0].shape
    kinds = len(factors)

    def body(p_ref, norm_ref, *refs):
        xs, own_refs, other_refs, outs = refs[:4], refs[4:8], refs[8:10], refs[10:]
        deep = own_refs[0].shape[0] - GATE_ROWS
        tall = deep + GATE_ROWS
        r = norm_ref[...]
        lane = lax.broadcasted_iota(jnp.int32, (GATE_ROWS, HD), 1)
        first_half = (lane < rows) == (p_ref[0] == 0)
        slabs = []
        for b in range(4):
            at = pl.ds(pl.multiple_of(p_ref[5 + b] * deep, deep), deep)
            slabs.append(
                jnp.concatenate(
                    [ref[i, :, at] for ref in xs for i in range(ref.shape[0])], axis=0
                )
            )
        own = [ref[:deep, cols] for ref in own_refs]
        other = [other_refs[0][:deep, cols]]
        other += [other_refs[1][n * tall : n * tall + deep, cols] for n in range(3)]
        for ref, ws, head in (
            (own_refs[0], own, p_ref[0]),
            (other_refs[0], other, 1 - p_ref[0]),
        ):
            y = jnp.dot(slabs[0], ws[0], preferred_element_type=F32)
            for b in range(1, 4):
                y = y + jnp.dot(slabs[b], ws[b], preferred_element_type=F32)
            y = y * r
            if not split:
                for a in range(4):
                    to = p_ref[1 + a]
                    g = ref[
                        deep:,
                        pl.ds(pl.multiple_of(to * 2 * rows, 2 * rows), 2 * rows),
                    ].astype(F32)
                    turned = pltpu.roll(g, rows, 1)
                    twice = jnp.where(first_half, g, turned).astype(BF16)
                    for i in range(seqs):
                        outs[0][to, i, head, 2 * rows :] = (
                            twice if i == 0 else jnp.roll(twice, -i * 8, 0)
                        )
            for kind, factor in enumerate(factors):
                part = y[:, kind * HD : (kind + 1) * HD]
                if factor != 1.0:
                    part = part * factor
                part = part.astype(BF16)
                for a in range(4):
                    for i in range(seqs):
                        at = (a * seqs + i) * rows
                        if split:
                            outs[a][kind, 0, i, head] = part[at : at + rows]
                        else:
                            outs[0][p_ref[1 + a], i, head, kind * rows : (kind + 1) * rows] = part[
                                at : at + rows
                            ]

    cols = slice(half * kinds * HD, (half + 1) * kinds * HD)
    if split:
        shapes = [(kinds, 1, seqs, 2, rows, HD)] * 4
    else:
        shapes = [(4, seqs, 2, kinds * rows + GATE_ROWS, HD)]
    outs = pl.pallas_call(
        body,
        in_specs=[whole(pltpu.SMEM)] + [whole()] * 11,
        out_specs=[whole()] * len(shapes),
        out_shape=[jax.ShapeDtypeStruct(sh, BF16) for sh in shapes],
        compiler_params=params(),
        name="project",
    )(places, norm, *rows_of, *own, *other)
    return outs


def attend(places, q, own, other):
    blocks, rows, _ = q.shape
    span = 8 * rows
    group = 4
    tall = group * rows
    count = blocks // group
    wide = WIDE

    def body(p_ref, q_ref, *refs):
        kvs, (out_ref, acc_ref, top_ref) = refs[:7], refs[7:]
        ones = jnp.ones((wide * span, HD), BF16)
        lane = lax.broadcasted_iota(jnp.int32, (1, HD), 1)
        left = lane < rows
        c = p_ref[0]
        bases = [(2 * p_ref[1 + n] + c) * rows for n in range(4)]
        bases += [(2 * p_ref[1 + n] + 1 - c) * rows for n in range(4)]
        key_at = jnp.concatenate(
            [
                jnp.where(left, lane + bases[n], lane - rows + bases[n + 1])
                for n in range(0, 8, 2)
            ],
            axis=1,
        )
        key_at = jnp.concatenate([key_at + n * span for n in range(wide)], axis=1)
        row = lax.broadcasted_iota(jnp.int32, (tall, 1), 0)
        query_at = (row // rows) * span + row % rows + bases[0]

        def blocks_of(s, late, at):
            far = kvs[4][s - blocks // 2, at] if late else kvs[3][s, at]
            return [kvs[0][s, at], kvs[1][s, at], kvs[2][s, at], far, kvs[5][s, at]] + [
                kvs[6][s + n * blocks, at] for n in range(3)
            ]

        def several(s, late, at):
            return [p for n in range(wide) for p in blocks_of(s + n, late, at)]

        def gates(s, late):
            parts = several(s, late, slice(2 * rows, 2 * rows + GATE_ROWS))
            parts = [jnp.sum(part.astype(F32)[:3], axis=0, keepdims=True) for part in parts]
            return LOG2E * jnp.concatenate(
                [jnp.where(left, parts[n], parts[n + 1]) for n in range(0, 8 * wide, 2)], axis=1
            )

        def step(s, first_group, fresh, late):
            k = jnp.concatenate(several(s, late, slice(0, rows)), axis=0)
            v = jnp.concatenate(several(s, late, slice(rows, 2 * rows)), axis=0)
            v = jnp.concatenate([v, ones], axis=1)
            gate = gates(s, late)
            for g in range(first_group, count):
                at = pl.ds(g * tall, tall)
                qt = q_ref[g * group : (g + 1) * group].reshape(tall, HD)
                sc = lax.dot_general(
                    qt, k, (((1,), (1,)), ((), ())), preferred_element_type=F32
                )
                sc = sc - gate
                if g == first_group:
                    sc = jnp.where(key_at + (s - g * group) * span <= query_at, sc, MASKED)
                new = jnp.max(sc, axis=1, keepdims=True)
                if fresh:
                    p = jnp.exp2(sc - new).astype(BF16)
                    acc_ref[at] = jnp.dot(p, v, preferred_element_type=F32)
                else:
                    top = top_ref[at]
                    new = jnp.maximum(top, new)
                    p = jnp.exp2(sc - new).astype(BF16)
                    acc_ref[at] = acc_ref[at] * jnp.exp2(top - new) + jnp.dot(
                        p, v, preferred_element_type=F32
                    )
                top_ref[at] = new

        step(0, 0, True, False)
        for r in range(count):

            def loop(n, carry, r=r):
                step(n * wide, r, False, 2 * r >= count)
                return carry

            lax.fori_loop(max(1, r * group // wide), (r + 1) * group // wide, loop, 0)
        for g in range(count):
            acc = acc_ref[g * tall : (g + 1) * tall]
            out_ref[g * group : (g + 1) * group] = (
                (acc[:, :HD] / acc[:, HD:]).astype(BF16).reshape(group, rows, HD)
            )

    return pl.pallas_call(
        body,
        in_specs=[whole(pltpu.SMEM)] + [whole()] * 8,
        out_specs=whole(),
        out_shape=jax.ShapeDtypeStruct(q.shape, BF16),
        scratch_shapes=[
            pltpu.VMEM((blocks * rows, 2 * HD), F32),
            pltpu.VMEM((blocks * rows, 1), F32),
        ],
        compiler_params=params(),
        name="attend",
    )(places, q, *own, *other)


def pool(first, rows_in, border, mix, scale):
    nx, seqs, two, rows, _ = rows_in.shape
    edge = border.shape[3]

    def body(first_ref, in_ref, edge_ref, mix_ref, scale_ref, out_ref):
        at = first_ref[0] + lax.broadcasted_iota(jnp.int32, (rows, 1), 0) + 1
        for x in range(nx):
            for c in range(two):
                group = 2 * x + c
                width = 2 ** (1 + group % 4)
                inverse = 1.0 / jnp.minimum(at, width).astype(F32)
                parts = []
                for i in range(seqs):
                    own = in_ref[x, i, c].astype(F32)
                    total = jnp.concatenate([edge_ref[x, i, c].astype(F32), own], axis=0)
                    by = 1
                    while by < width:
                        total = total + pltpu.roll(total, by, 0)
                        by *= 2
                    parts.append((total[edge:] * inverse - own).astype(BF16))
                mixed = jnp.dot(
                    jnp.concatenate(parts, axis=0), mix_ref[group], preferred_element_type=F32
                )
                mixed = (mixed * scale_ref[group : group + 1, :]).astype(BF16)
                for i in range(seqs):
                    out_ref[x, i, c] = mixed[i * rows : (i + 1) * rows]

    return pl.pallas_call(
        body,
        in_specs=[whole(pltpu.SMEM)] + [whole()] * 4,
        out_specs=whole(),
        out_shape=jax.ShapeDtypeStruct(rows_in.shape, BF16),
        compiler_params=params(),
        name="pool",
    )(first, rows_in, border, mix, scale)


def finish(places, pooled, attn, pooled_pair, attn_pair, w):
    nx, seqs, _, rows, _ = pooled.shape
    ny, deep, wide = w[0].shape
    own = seqs * rows

    def body(p_ref, pool_ref, attn_ref, pool_pair_ref, attn_pair_ref, *refs):
        out_ref, pair_ref = refs[5:]
        late = pl.program_id(0) >= ny // 2
        c = p_ref[0]
        total = jnp.zeros((2 * own, wide), F32)
        for a in range(nx):
            x = p_ref[1 + a]
            left = jnp.concatenate(
                [
                    jnp.concatenate(
                        [ref[x, i, c] for ref in two for i in range(seqs)], axis=0
                    )
                    for two in ((pool_ref, pool_pair_ref), (attn_ref, attn_pair_ref))
                ],
                axis=1,
            )
            right = refs[a][0] if a < 3 else jnp.where(late, refs[4][0], refs[3][0])
            total = total + jnp.dot(left, right, preferred_element_type=F32)
        out_ref[...] = total[:own].reshape(seqs, rows, wide)
        pair_ref[...] = total[own:].astype(BF16).reshape(seqs, rows, wide)

    half = ny // 2
    shape = (1, deep, wide)
    specs = [pl.BlockSpec(shape, lambda j: (j, 0, 0))] * 3 + [
        pl.BlockSpec(shape, lambda j: (jnp.minimum(j, half - 1), 0, 0)),
        pl.BlockSpec(shape, lambda j: (jnp.maximum(j - half, 0), 0, 0)),
    ]
    out_spec = pl.BlockSpec((seqs, rows, wide), lambda j: (0, 0, j))
    out = (seqs, rows, ny * wide)
    return pl.pallas_call(
        body,
        grid=(ny,),
        in_specs=[whole(pltpu.SMEM)] + [whole()] * 4 + specs,
        out_specs=[out_spec, out_spec],
        out_shape=[jax.ShapeDtypeStruct(out, F32), jax.ShapeDtypeStruct(out, BF16)],
        compiler_params=params(),
        name="finish",
    )(places, pooled, attn, pooled_pair, attn_pair, *w)


def after(x, *others):
    return lax.optimization_barrier((x,) + others)[0]


def placed(pieces, where, dim):
    shape = list(pieces[0].shape)
    shape[dim] = len(pieces)
    out = jnp.zeros(shape, pieces[0].dtype)
    for piece, at in zip(pieces, where):
        out = lax.dynamic_update_slice_in_dim(out, piece, at, dim)
    return out


def on_device(
    tokens,
    norm_gain,
    w_pool_in,
    pool_mix,
    pool_scale,
    w_query,
    w_key,
    w_value,
    gate_cache,
    w_out_pool,
    w_out_attn,
):
    z = lax.axis_index("sp")
    x = lax.axis_index("tp_0")
    y = lax.axis_index("fs")
    c = lax.axis_index("tp_1")
    planes = lax.axis_size("sp")
    chunks = lax.axis_size("tp_0")
    seqs, rows, _ = tokens.shape
    block = rows * chunks * 2
    seen = [x, (x + 3) % 4, (x + 1) % 4, (x + 2) % 4]
    deeps = [y, (y + 3) % 4, (y + 1) % 4, (y + 2) % 4]
    places = jnp.stack([c] + seen + deeps).astype(jnp.int32)

    deep = w_key.shape[0]
    gain = lax.dynamic_slice_in_dim(norm_gain, y * deep, deep, 0)
    all_rows = ring_in_three(tokens, "tp_0")
    norm = factors_of(all_rows)
    weights = jnp.concatenate([w_key, w_value, w_query, w_pool_in], axis=1)
    weights = (weights.astype(F32) * gain[:, None]).astype(BF16)
    here = lax.dynamic_slice_in_dim(gate_cache[:, 0], z * block, block, 1)
    high = lax.reduce_precision(here, 8, 7)
    rest = here - high
    middle = lax.reduce_precision(rest, 8, 7)
    parts = jnp.stack([high, middle, rest - middle], axis=1).astype(BF16)
    parts = jnp.pad(parts, ((0, 0), (0, 5), (0, 0))).reshape(GATE_ROWS, block)
    own_w = ring_in_three(jnp.concatenate([weights, parts], axis=0), "fs")
    other_w = sibling(own_w[0])
    other_w = (other_w, sibling(jnp.concatenate(own_w[1:], axis=0)))

    (kv,) = project(places, norm, all_rows, own_w, other_w, 0, (1.0, 1.0), False)
    kv_here = lax.all_to_all(kv, "tp_0", 0, 0, tiled=True)
    kv = lax.all_to_all(kv_here.reshape(planes, 2 * rows + GATE_ROWS, HD), "sp", 0, 0, tiled=True)
    qp = project(
        places, norm, all_rows, own_w, other_w, 1, (HD**-0.5 * LOG2E, 1.0), True
    )
    got = [qp[0]]
    for piece, by in zip(qp[1:], (-1, 1, 2)):
        got.append(
            lax.ppermute(piece, "tp_0", [(i, (i + by) % 4) for i in range(4)])
        )
    came = [x, (x + 1) % 4, (x + 3) % 4, (x + 2) % 4]
    qp = placed(got, came, 1)

    q = after(qp[0].reshape(planes, rows, HD), kv)
    q = lax.all_to_all(q, "sp", 0, 0, tiled=True)
    pool_in = qp[1]
    total = planes * chunks * 2
    border = lax.ppermute(
        pool_in[:, :, :, rows - 16 :], SP_TP, [(i, i + 1) for i in range(total - 1)]
    )
    first = (z * block + (2 * x + c) * rows).reshape(1).astype(jnp.int32)
    pooled = pool(first, pool_in, border, pool_mix, pool_scale.reshape(-1, HD))
    pooled_pair = sibling(pooled)

    kv_own = ring_of_four(kv, "tp_0")
    kv_other = sibling(kv)
    kv_other = (kv_other, sibling(jnp.concatenate(kv_own[1:], axis=0)))

    out_w = jnp.concatenate([w_out_pool, w_out_attn], axis=0)
    o = ring_in_three(after(out_w, own_w[1]), "fs")
    o = placed([w[None] for w in o], deeps, 0)
    out_near = hops(after(o, kv_here), "tp_0")

    attn = attend(places, q, kv_own, kv_other)
    out_near = lax.optimization_barrier((*out_near, attn))[:2]
    out_own = (o, *out_near, *relays(*out_near, "tp_0"))
    attn = lax.all_to_all(attn, "sp", 0, 0, tiled=True)
    attn = attn.reshape(chunks, seqs, 2, rows, HD)
    mine, theirs = finish(
        places, pooled, attn, pooled_pair, sibling(attn), out_own
    )
    return (mine + sibling(theirs).astype(F32)).astype(BF16)


def solution(mesh):
    torus = Mesh(
        mesh.devices.reshape(mesh.shape["sp"], mesh.shape["fs"], 4, 2), ("sp", "fs", "tp_0", "tp_1")
    )
    return jax.shard_map(
        on_device,
        mesh=torus,
        in_specs=(
            P("fs", SP_TP, None),
            P(),
            P("fs", TP),
            P(),
            P(),
            P("fs", TP),
            P("fs", TP),
            P("fs", TP),
            P("fs", TP, None),
            P(TP, "fs"),
            P(TP, "fs"),
        ),
        out_specs=P("fs", SP_TP, None),
        check_vma=False,
    )
```

```python
import jax
import jax.numpy as jnp
from jax import lax
from jax.experimental import pallas as pl
from jax.experimental.pallas import tpu as pltpu
from jax.sharding import Mesh
from jax.sharding import PartitionSpec as P

HD = 128
TP = ("tp_0", "tp_1")
SP_TP = ("sp", "tp_0", "tp_1")
EPS = 1e-06
MASKED = -1e30
GATE_ROWS = 16
WIDE = 4
LOG2E = 1.4426950408889634
F32 = jnp.float32
BF16 = jnp.bfloat16
VMEM_LIMIT = 56 * 1024 * 1024


def params(**kw):
    return pltpu.CompilerParams(vmem_limit_bytes=VMEM_LIMIT, **kw)


def whole(memory=pltpu.VMEM):
    return pl.BlockSpec(memory_space=memory)


def sibling(x):
    return lax.ppermute(x, "tp_1", [(0, 1), (1, 0)])


UP = [(i, (i + 1) % 4) for i in range(4)]
DOWN = [(i, (i - 1) % 4) for i in range(4)]


def hops(x, axis):
    return lax.ppermute(x, axis, UP), lax.ppermute(x, axis, DOWN)


def relays(before, after, axis):
    half = before.shape[0] // 2
    return lax.ppermute(before[:half], axis, UP), lax.ppermute(after[half:], axis, DOWN)


def ring_of_four(x, axis):
    near = hops(x, axis)
    return (x, *near, *relays(*near, axis))


def ring_in_three(x, axis):
    near = hops(x, axis)
    return (x, *near, lax.ppermute(near[0], axis, UP))


def project(places, rows_of, own, other, half, factors, split):
    seqs, rows, depth = rows_of[0].shape
    kinds = len(factors)

    def body(p_ref, *refs):
        xs, own_refs, other_refs, outs = refs[:4], refs[4:9], refs[9:11], refs[11:]
        deep = own_refs[0].shape[0] - GATE_ROWS
        tall = deep + GATE_ROWS
        lane = lax.broadcasted_iota(jnp.int32, (GATE_ROWS, HD), 1)
        first_half = (lane < rows) == (p_ref[0] == 0)
        slabs = []
        for b in range(4):
            at = pl.ds(pl.multiple_of(p_ref[5 + b] * deep, deep), deep)
            slabs.append(
                jnp.concatenate(
                    [ref[i, :, at] for ref in xs for i in range(ref.shape[0])], axis=0
                )
            )
        squares = jnp.zeros((4 * seqs * rows, 1), F32)
        for slab in slabs:
            wide = slab.astype(F32)
            squares = squares + jnp.sum(wide * wide, axis=-1, keepdims=True)
        r = lax.rsqrt(squares * (1.0 / depth) + EPS)
        own = [ref[:deep, cols] for ref in own_refs[:3]]
        far = jnp.concatenate([ref[:, cols] for ref in own_refs[3:]], axis=0)
        own.append(far[:deep])
        other = [other_refs[0][:deep, cols]]
        other += [other_refs[1][n * tall : n * tall + deep, cols] for n in range(3)]
        for ref, ws, head in (
            (own_refs[0], own, p_ref[0]),
            (other_refs[0], other, 1 - p_ref[0]),
        ):
            y = jnp.dot(slabs[0], ws[0], preferred_element_type=F32)
            for b in range(1, 4):
                y = y + jnp.dot(slabs[b], ws[b], preferred_element_type=F32)
            y = y * r
            if not split:
                for a in range(4):
                    to = p_ref[1 + a]
                    g = ref[
                        deep:,
                        pl.ds(pl.multiple_of(to * 2 * rows, 2 * rows), 2 * rows),
                    ].astype(F32)
                    turned = pltpu.roll(g, rows, 1)
                    twice = jnp.where(first_half, g, turned).astype(BF16)
                    for i in range(seqs):
                        outs[0][to, i, head, 2 * rows :] = (
                            twice if i == 0 else jnp.roll(twice, -i * 8, 0)
                        )
            for kind, factor in enumerate(factors):
                part = y[:, kind * HD : (kind + 1) * HD]
                if factor != 1.0:
                    part = part * factor
                part = part.astype(BF16)
                for a in range(4):
                    for i in range(seqs):
                        at = (a * seqs + i) * rows
                        if split:
                            outs[a][kind, 0, i, head] = part[at : at + rows]
                        else:
                            outs[0][p_ref[1 + a], i, head, kind * rows : (kind + 1) * rows] = part[
                                at : at + rows
                            ]

    cols = slice(half * kinds * HD, (half + 1) * kinds * HD)
    if split:
        shapes = [(kinds, 1, seqs, 2, rows, HD)] * 4
    else:
        shapes = [(4, seqs, 2, kinds * rows + GATE_ROWS, HD)]
    outs = pl.pallas_call(
        body,
        in_specs=[whole(pltpu.SMEM)] + [whole()] * 11,
        out_specs=[whole()] * len(shapes),
        out_shape=[jax.ShapeDtypeStruct(sh, BF16) for sh in shapes],
        compiler_params=params(),
        name="project",
    )(places, *rows_of, *own, *other)
    return outs


def attend(places, q, own, other):
    blocks, rows, _ = q.shape
    span = 8 * rows
    group = 4
    tall = group * rows
    count = blocks // group
    wide = WIDE

    def body(p_ref, q_ref, *refs):
        kvs, (out_ref, acc_ref, top_ref) = refs[:7], refs[7:]
        ones = jnp.ones((wide * span, HD), BF16)
        lane = lax.broadcasted_iota(jnp.int32, (1, HD), 1)
        left = lane < rows
        c = p_ref[0]
        bases = [(2 * p_ref[1 + n] + c) * rows for n in range(4)]
        bases += [(2 * p_ref[1 + n] + 1 - c) * rows for n in range(4)]
        key_at = jnp.concatenate(
            [
                jnp.where(left, lane + bases[n], lane - rows + bases[n + 1])
                for n in range(0, 8, 2)
            ],
            axis=1,
        )
        key_at = jnp.concatenate([key_at + n * span for n in range(wide)], axis=1)
        row = lax.broadcasted_iota(jnp.int32, (tall, 1), 0)
        query_at = (row // rows) * span + row % rows + bases[0]

        def blocks_of(s, late, at):
            far = kvs[4][s - blocks // 2, at] if late else kvs[3][s, at]
            return [kvs[0][s, at], kvs[1][s, at], kvs[2][s, at], far, kvs[5][s, at]] + [
                kvs[6][s + n * blocks, at] for n in range(3)
            ]

        def several(s, late, at):
            return [p for n in range(wide) for p in blocks_of(s + n, late, at)]

        def gates(s, late):
            parts = several(s, late, slice(2 * rows, 2 * rows + GATE_ROWS))
            parts = [jnp.sum(part.astype(F32)[:3], axis=0, keepdims=True) for part in parts]
            return LOG2E * jnp.concatenate(
                [jnp.where(left, parts[n], parts[n + 1]) for n in range(0, 8 * wide, 2)], axis=1
            )

        def step(s, first_group, fresh, late):
            k = jnp.concatenate(several(s, late, slice(0, rows)), axis=0)
            v = jnp.concatenate(several(s, late, slice(rows, 2 * rows)), axis=0)
            v = jnp.concatenate([v, ones], axis=1)
            gate = gates(s, late)
            for g in range(first_group, count):
                at = pl.ds(g * tall, tall)
                qt = q_ref[g * group : (g + 1) * group].reshape(tall, HD)
                sc = lax.dot_general(
                    qt, k, (((1,), (1,)), ((), ())), preferred_element_type=F32
                )
                sc = sc - gate
                if g == first_group:
                    sc = jnp.where(key_at + (s - g * group) * span <= query_at, sc, MASKED)
                new = jnp.max(sc, axis=1, keepdims=True)
                if fresh:
                    p = jnp.exp2(sc - new).astype(BF16)
                    acc_ref[at] = jnp.dot(p, v, preferred_element_type=F32)
                else:
                    top = top_ref[at]
                    new = jnp.maximum(top, new)
                    p = jnp.exp2(sc - new).astype(BF16)
                    acc_ref[at] = acc_ref[at] * jnp.exp2(top - new) + jnp.dot(
                        p, v, preferred_element_type=F32
                    )
                top_ref[at] = new

        step(0, 0, True, False)
        for r in range(count):

            def loop(n, carry, r=r):
                step(n * wide, r, False, 2 * r >= count)
                return carry

            lax.fori_loop(max(1, r * group // wide), (r + 1) * group // wide, loop, 0)
        for g in range(count):
            acc = acc_ref[g * tall : (g + 1) * tall]
            out_ref[g * group : (g + 1) * group] = (
                (acc[:, :HD] / acc[:, HD:]).astype(BF16).reshape(group, rows, HD)
            )

    return pl.pallas_call(
        body,
        in_specs=[whole(pltpu.SMEM)] + [whole()] * 8,
        out_specs=whole(),
        out_shape=jax.ShapeDtypeStruct(q.shape, BF16),
        scratch_shapes=[
            pltpu.VMEM((blocks * rows, 2 * HD), F32),
            pltpu.VMEM((blocks * rows, 1), F32),
        ],
        compiler_params=params(),
        name="attend",
    )(places, q, *own, *other)


def pool(first, rows_in, border, mix, scale):
    nx, seqs, two, rows, _ = rows_in.shape
    edge = border.shape[3]

    def body(first_ref, in_ref, edge_ref, mix_ref, scale_ref, out_ref):
        at = first_ref[0] + lax.broadcasted_iota(jnp.int32, (rows, 1), 0) + 1
        for x in range(nx):
            for c in range(two):
                group = 2 * x + c
                width = 2 ** (1 + group % 4)
                inverse = 1.0 / jnp.minimum(at, width).astype(F32)
                parts = []
                for i in range(seqs):
                    own = in_ref[x, i, c].astype(F32)
                    total = jnp.concatenate([edge_ref[x, i, c].astype(F32), own], axis=0)
                    by = 1
                    while by < width:
                        total = total + pltpu.roll(total, by, 0)
                        by *= 2
                    parts.append((total[edge:] * inverse - own).astype(BF16))
                mixed = jnp.dot(
                    jnp.concatenate(parts, axis=0), mix_ref[group], preferred_element_type=F32
                )
                mixed = (mixed * scale_ref[group : group + 1, :]).astype(BF16)
                for i in range(seqs):
                    out_ref[x, i, c] = mixed[i * rows : (i + 1) * rows]

    return pl.pallas_call(
        body,
        in_specs=[whole(pltpu.SMEM)] + [whole()] * 4,
        out_specs=whole(),
        out_shape=jax.ShapeDtypeStruct(rows_in.shape, BF16),
        compiler_params=params(),
        name="pool",
    )(first, rows_in, border, mix, scale)


def finish(places, pooled, attn, own, other):
    nx, seqs, _, rows, _ = pooled.shape
    ny, deep, wide = own[0].shape

    def body(p_ref, pool_ref, attn_ref, *refs):
        out_ref = refs[10]
        late = pl.program_id(0) >= ny // 2
        total = jnp.zeros((seqs * rows, wide), F32)
        for side, c in ((refs[:5], p_ref[0]), (refs[5:10], 1 - p_ref[0])):
            for a in range(nx):
                x = p_ref[1 + a]
                left = jnp.concatenate(
                    [
                        jnp.concatenate([pool_ref[x, i, c] for i in range(seqs)], axis=0),
                        jnp.concatenate([attn_ref[x, i, c] for i in range(seqs)], axis=0),
                    ],
                    axis=1,
                )
                right = side[a][0] if a < 3 else jnp.where(late, side[4][0], side[3][0])
                total = total + jnp.dot(left, right, preferred_element_type=F32)
        out_ref[...] = total.astype(BF16).reshape(seqs, rows, wide)

    half = ny // 2
    shape = (1, deep, wide)
    specs = [pl.BlockSpec(shape, lambda j: (j, 0, 0))] * 3 + [
        pl.BlockSpec(shape, lambda j: (jnp.minimum(j, half - 1), 0, 0)),
        pl.BlockSpec(shape, lambda j: (jnp.maximum(j - half, 0), 0, 0)),
    ]
    return pl.pallas_call(
        body,
        grid=(ny,),
        in_specs=[whole(pltpu.SMEM), whole(), whole()] + specs + specs,
        out_specs=pl.BlockSpec((seqs, rows, wide), lambda j: (0, 0, j)),
        out_shape=jax.ShapeDtypeStruct((seqs, rows, ny * wide), BF16),
        compiler_params=params(),
        name="finish",
    )(places, pooled, attn, *own, *other)


def after(x, *others):
    return lax.optimization_barrier((x,) + others)[0]


def placed(pieces, where, dim):
    shape = list(pieces[0].shape)
    shape[dim] = len(pieces)
    out = jnp.zeros(shape, pieces[0].dtype)
    for piece, at in zip(pieces, where):
        out = lax.dynamic_update_slice_in_dim(out, piece, at, dim)
    return out


def on_device(
    tokens,
    norm_gain,
    w_pool_in,
    pool_mix,
    pool_scale,
    w_query,
    w_key,
    w_value,
    gate_cache,
    w_out_pool,
    w_out_attn,
):
    z = lax.axis_index("sp")
    x = lax.axis_index("tp_0")
    y = lax.axis_index("fs")
    c = lax.axis_index("tp_1")
    planes = lax.axis_size("sp")
    chunks = lax.axis_size("tp_0")
    seqs, rows, _ = tokens.shape
    block = rows * chunks * 2
    seen = [x, (x + 3) % 4, (x + 1) % 4, (x + 2) % 4]
    deeps = [y, (y + 3) % 4, (y + 1) % 4, (y + 2) % 4]
    places = jnp.stack([c] + seen + deeps).astype(jnp.int32)

    deep = w_key.shape[0]
    gain = lax.dynamic_slice_in_dim(norm_gain, y * deep, deep, 0)
    all_rows = ring_in_three(tokens, "tp_0")
    weights = jnp.concatenate([w_key, w_value, w_query, w_pool_in], axis=1)
    weights = (weights.astype(F32) * gain[:, None]).astype(BF16)
    here = lax.dynamic_slice_in_dim(gate_cache[:, 0], z * block, block, 1)
    high = lax.reduce_precision(here, 8, 7)
    rest = here - high
    middle = lax.reduce_precision(rest, 8, 7)
    parts = jnp.stack([high, middle, rest - middle], axis=1).astype(BF16)
    parts = jnp.pad(parts, ((0, 0), (0, 5), (0, 0))).reshape(GATE_ROWS, block)
    own_w = ring_of_four(jnp.concatenate([weights, parts], axis=0), "fs")
    other_w = sibling(own_w[0])
    other_w = (other_w, sibling(jnp.concatenate(own_w[1:], axis=0)))

    (kv,) = project(places, all_rows, own_w, other_w, 0, (1.0, 1.0), False)
    kv_here = lax.all_to_all(kv, "tp_0", 0, 0, tiled=True)
    kv = lax.all_to_all(kv_here.reshape(planes, 2 * rows + GATE_ROWS, HD), "sp", 0, 0, tiled=True)
    qp = project(
        places, all_rows, own_w, other_w, 1, (HD**-0.5 * LOG2E, 1.0), True
    )
    got = [qp[0]]
    for piece, by in zip(qp[1:], (-1, 1, 2)):
        got.append(
            lax.ppermute(piece, "tp_0", [(i, (i + by) % 4) for i in range(4)])
        )
    came = [x, (x + 1) % 4, (x + 3) % 4, (x + 2) % 4]
    qp = placed(got, came, 1)

    q = after(qp[0].reshape(planes, rows, HD), kv)
    q = lax.all_to_all(q, "sp", 0, 0, tiled=True)
    pool_in = qp[1]
    total = planes * chunks * 2
    border = lax.ppermute(
        pool_in[:, :, :, rows - 16 :], SP_TP, [(i, i + 1) for i in range(total - 1)]
    )
    first = (z * block + (2 * x + c) * rows).reshape(1).astype(jnp.int32)
    pooled = pool(first, pool_in, border, pool_mix, pool_scale.reshape(-1, HD))

    kv_own = ring_of_four(kv, "tp_0")
    kv_other = sibling(kv)
    kv_other = (kv_other, sibling(jnp.concatenate(kv_own[1:], axis=0)))

    out_w = jnp.concatenate([w_out_pool, w_out_attn], axis=0)
    o = ring_in_three(after(out_w, own_w[1]), "fs")
    o = placed([w[None] for w in o], deeps, 0)
    out_near = hops(after(o, kv_here), "tp_0")

    attn = attend(places, q, kv_own, kv_other)
    out_near = lax.optimization_barrier((*out_near, attn))[:2]
    out_own = (o, *out_near, *relays(*out_near, "tp_0"))
    out_other = [sibling(piece) for piece in out_own[1:3]]
    out_other += [sibling(piece) for piece in out_own[3:]]
    out_other = [sibling(o)] + out_other
    attn = lax.all_to_all(attn, "sp", 0, 0, tiled=True)
    attn = attn.reshape(chunks, seqs, 2, rows, HD)
    return finish(places, pooled, attn, out_own, out_other)


def solution(mesh):
    torus = Mesh(
        mesh.devices.reshape(mesh.shape["sp"], mesh.shape["fs"], 4, 2), ("sp", "fs", "tp_0", "tp_1")
    )
    return jax.shard_map(
        on_device,
        mesh=torus,
        in_specs=(
            P("fs", SP_TP, None),
            P(),
            P("fs", TP),
            P(),
            P(),
            P("fs", TP),
            P("fs", TP),
            P("fs", TP),
            P("fs", TP, None),
            P(TP, "fs"),
            P(TP, "fs"),
        ),
        out_specs=P("fs", SP_TP, None),
        check_vma=False,
    )
```

```python
import jax
import jax.numpy as jnp
from jax import lax
from jax.experimental import pallas as pl
from jax.experimental.pallas import tpu as pltpu
from jax.sharding import Mesh
from jax.sharding import PartitionSpec as P

HD = 128
TP = ("tp_0", "tp_1")
SP_TP = ("sp", "tp_0", "tp_1")
EPS = 1e-06
MASKED = -1e30
GATE_ROWS = 16
WIDE = 4
LOG2E = 1.4426950408889634
F32 = jnp.float32
BF16 = jnp.bfloat16
VMEM_LIMIT = 56 * 1024 * 1024


def params(**kw):
    return pltpu.CompilerParams(vmem_limit_bytes=VMEM_LIMIT, **kw)


def whole(memory=pltpu.VMEM):
    return pl.BlockSpec(memory_space=memory)


def sibling(x):
    return lax.ppermute(x, "tp_1", [(0, 1), (1, 0)])


UP = [(i, (i + 1) % 4) for i in range(4)]
DOWN = [(i, (i - 1) % 4) for i in range(4)]


def hops(x, axis):
    return lax.ppermute(x, axis, UP), lax.ppermute(x, axis, DOWN)


def relays(before, after, axis):
    half = before.shape[0] // 2
    return lax.ppermute(before[:half], axis, UP), lax.ppermute(after[half:], axis, DOWN)


def ring_of_four(x, axis):
    near = hops(x, axis)
    return (x, *near, *relays(*near, axis))


def ring_in_three(x, axis):
    near = hops(x, axis)
    return (x, *near, lax.ppermute(near[0], axis, UP))


def project(places, rows_of, own, other, half, factors, split):
    seqs, rows, depth = rows_of[0].shape
    kinds = len(factors)

    def body(p_ref, *refs):
        xs, own_refs, other_refs, outs = refs[:5], refs[5:10], refs[10:12], refs[12:]
        deep = own_refs[0].shape[0] - GATE_ROWS
        tall = deep + GATE_ROWS
        lane = lax.broadcasted_iota(jnp.int32, (GATE_ROWS, HD), 1)
        first_half = (lane < rows) == (p_ref[0] == 0)
        slabs = []
        for b in range(4):
            at = pl.ds(pl.multiple_of(p_ref[5 + b] * deep, deep), deep)
            slabs.append(
                jnp.concatenate(
                    [ref[i, :, at] for ref in xs for i in range(ref.shape[0])], axis=0
                )
            )
        squares = jnp.zeros((4 * seqs * rows, 1), F32)
        for slab in slabs:
            wide = slab.astype(F32)
            squares = squares + jnp.sum(wide * wide, axis=-1, keepdims=True)
        r = lax.rsqrt(squares * (1.0 / depth) + EPS)
        own = [ref[:deep, cols] for ref in own_refs[:3]]
        far = jnp.concatenate([ref[:, cols] for ref in own_refs[3:]], axis=0)
        own.append(far[:deep])
        other = [other_refs[0][:deep, cols]]
        other += [other_refs[1][n * tall : n * tall + deep, cols] for n in range(3)]
        for ref, ws, head in (
            (own_refs[0], own, p_ref[0]),
            (other_refs[0], other, 1 - p_ref[0]),
        ):
            y = jnp.dot(slabs[0], ws[0], preferred_element_type=F32)
            for b in range(1, 4):
                y = y + jnp.dot(slabs[b], ws[b], preferred_element_type=F32)
            y = y * r
            if not split:
                for a in range(4):
                    to = p_ref[1 + a]
                    g = ref[
                        deep:,
                        pl.ds(pl.multiple_of(to * 2 * rows, 2 * rows), 2 * rows),
                    ].astype(F32)
                    turned = pltpu.roll(g, rows, 1)
                    twice = jnp.where(first_half, g, turned).astype(BF16)
                    for i in range(seqs):
                        outs[0][to, i, head, 2 * rows :] = (
                            twice if i == 0 else jnp.roll(twice, -i * 8, 0)
                        )
            for kind, factor in enumerate(factors):
                part = y[:, kind * HD : (kind + 1) * HD]
                if factor != 1.0:
                    part = part * factor
                part = part.astype(BF16)
                for a in range(4):
                    for i in range(seqs):
                        at = (a * seqs + i) * rows
                        if split:
                            outs[a][kind, 0, i, head] = part[at : at + rows]
                        else:
                            outs[0][p_ref[1 + a], i, head, kind * rows : (kind + 1) * rows] = part[
                                at : at + rows
                            ]

    cols = slice(half * kinds * HD, (half + 1) * kinds * HD)
    if split:
        shapes = [(kinds, 1, seqs, 2, rows, HD)] * 4
    else:
        shapes = [(4, seqs, 2, kinds * rows + GATE_ROWS, HD)]
    outs = pl.pallas_call(
        body,
        in_specs=[whole(pltpu.SMEM)] + [whole()] * 12,
        out_specs=[whole()] * len(shapes),
        out_shape=[jax.ShapeDtypeStruct(sh, BF16) for sh in shapes],
        compiler_params=params(),
        name="project",
    )(places, *rows_of, *own, *other)
    return outs


def attend(places, q, own, other):
    blocks, rows, _ = q.shape
    span = 8 * rows
    group = 4
    tall = group * rows
    count = blocks // group
    wide = WIDE

    def body(p_ref, q_ref, *refs):
        kvs, (out_ref, acc_ref, top_ref) = refs[:7], refs[7:]
        ones = jnp.ones((wide * span, HD), BF16)
        lane = lax.broadcasted_iota(jnp.int32, (1, HD), 1)
        left = lane < rows
        c = p_ref[0]
        bases = [(2 * p_ref[1 + n] + c) * rows for n in range(4)]
        bases += [(2 * p_ref[1 + n] + 1 - c) * rows for n in range(4)]
        key_at = jnp.concatenate(
            [
                jnp.where(left, lane + bases[n], lane - rows + bases[n + 1])
                for n in range(0, 8, 2)
            ],
            axis=1,
        )
        key_at = jnp.concatenate([key_at + n * span for n in range(wide)], axis=1)
        row = lax.broadcasted_iota(jnp.int32, (tall, 1), 0)
        query_at = (row // rows) * span + row % rows + bases[0]

        def blocks_of(s, late, at):
            far = kvs[4][s - blocks // 2, at] if late else kvs[3][s, at]
            return [kvs[0][s, at], kvs[1][s, at], kvs[2][s, at], far, kvs[5][s, at]] + [
                kvs[6][s + n * blocks, at] for n in range(3)
            ]

        def several(s, late, at):
            return [p for n in range(wide) for p in blocks_of(s + n, late, at)]

        def gates(s, late):
            parts = several(s, late, slice(2 * rows, 2 * rows + GATE_ROWS))
            parts = [jnp.sum(part.astype(F32)[:3], axis=0, keepdims=True) for part in parts]
            return LOG2E * jnp.concatenate(
                [jnp.where(left, parts[n], parts[n + 1]) for n in range(0, 8 * wide, 2)], axis=1
            )

        def step(s, first_group, fresh, late):
            k = jnp.concatenate(several(s, late, slice(0, rows)), axis=0)
            v = jnp.concatenate(several(s, late, slice(rows, 2 * rows)), axis=0)
            v = jnp.concatenate([v, ones], axis=1)
            gate = gates(s, late)
            for g in range(first_group, count):
                at = pl.ds(g * tall, tall)
                qt = q_ref[g * group : (g + 1) * group].reshape(tall, HD)
                sc = lax.dot_general(
                    qt, k, (((1,), (1,)), ((), ())), preferred_element_type=F32
                )
                sc = sc - gate
                if g == first_group:
                    sc = jnp.where(key_at + (s - g * group) * span <= query_at, sc, MASKED)
                new = jnp.max(sc, axis=1, keepdims=True)
                if fresh:
                    p = jnp.exp2(sc - new).astype(BF16)
                    acc_ref[at] = jnp.dot(p, v, preferred_element_type=F32)
                else:
                    top = top_ref[at]
                    new = jnp.maximum(top, new)
                    p = jnp.exp2(sc - new).astype(BF16)
                    acc_ref[at] = acc_ref[at] * jnp.exp2(top - new) + jnp.dot(
                        p, v, preferred_element_type=F32
                    )
                top_ref[at] = new

        step(0, 0, True, False)
        for r in range(count):

            def loop(n, carry, r=r):
                step(n * wide, r, False, 2 * r >= count)
                return carry

            lax.fori_loop(max(1, r * group // wide), (r + 1) * group // wide, loop, 0)
        for g in range(count):
            acc = acc_ref[g * tall : (g + 1) * tall]
            out_ref[g * group : (g + 1) * group] = (
                (acc[:, :HD] / acc[:, HD:]).astype(BF16).reshape(group, rows, HD)
            )

    return pl.pallas_call(
        body,
        in_specs=[whole(pltpu.SMEM)] + [whole()] * 8,
        out_specs=whole(),
        out_shape=jax.ShapeDtypeStruct(q.shape, BF16),
        scratch_shapes=[
            pltpu.VMEM((blocks * rows, 2 * HD), F32),
            pltpu.VMEM((blocks * rows, 1), F32),
        ],
        compiler_params=params(),
        name="attend",
    )(places, q, *own, *other)


def pool(first, rows_in, border, mix, scale):
    nx, seqs, two, rows, _ = rows_in.shape
    edge = border.shape[3]

    def body(first_ref, in_ref, edge_ref, mix_ref, scale_ref, out_ref):
        at = first_ref[0] + lax.broadcasted_iota(jnp.int32, (rows, 1), 0) + 1
        for x in range(nx):
            for c in range(two):
                group = 2 * x + c
                width = 2 ** (1 + group % 4)
                inverse = 1.0 / jnp.minimum(at, width).astype(F32)
                parts = []
                for i in range(seqs):
                    own = in_ref[x, i, c].astype(F32)
                    total = jnp.concatenate([edge_ref[x, i, c].astype(F32), own], axis=0)
                    by = 1
                    while by < width:
                        total = total + pltpu.roll(total, by, 0)
                        by *= 2
                    parts.append((total[edge:] * inverse - own).astype(BF16))
                mixed = jnp.dot(
                    jnp.concatenate(parts, axis=0), mix_ref[group], preferred_element_type=F32
                )
                mixed = (mixed * scale_ref[group : group + 1, :]).astype(BF16)
                for i in range(seqs):
                    out_ref[x, i, c] = mixed[i * rows : (i + 1) * rows]

    return pl.pallas_call(
        body,
        in_specs=[whole(pltpu.SMEM)] + [whole()] * 4,
        out_specs=whole(),
        out_shape=jax.ShapeDtypeStruct(rows_in.shape, BF16),
        compiler_params=params(),
        name="pool",
    )(first, rows_in, border, mix, scale)


def finish(places, pooled, attn, own, other):
    nx, seqs, _, rows, _ = pooled.shape
    ny, deep, wide = own[0].shape

    def body(p_ref, pool_ref, attn_ref, *refs):
        out_ref = refs[10]
        late = pl.program_id(0) >= ny // 2
        total = jnp.zeros((seqs * rows, wide), F32)
        for side, c in ((refs[:5], p_ref[0]), (refs[5:10], 1 - p_ref[0])):
            for a in range(nx):
                x = p_ref[1 + a]
                left = jnp.concatenate(
                    [
                        jnp.concatenate([pool_ref[x, i, c] for i in range(seqs)], axis=0),
                        jnp.concatenate([attn_ref[x, i, c] for i in range(seqs)], axis=0),
                    ],
                    axis=1,
                )
                right = side[a][0] if a < 3 else jnp.where(late, side[4][0], side[3][0])
                total = total + jnp.dot(left, right, preferred_element_type=F32)
        out_ref[...] = total.astype(BF16).reshape(seqs, rows, wide)

    half = ny // 2
    shape = (1, deep, wide)
    specs = [pl.BlockSpec(shape, lambda j: (j, 0, 0))] * 3 + [
        pl.BlockSpec(shape, lambda j: (jnp.minimum(j, half - 1), 0, 0)),
        pl.BlockSpec(shape, lambda j: (jnp.maximum(j - half, 0), 0, 0)),
    ]
    return pl.pallas_call(
        body,
        grid=(ny,),
        in_specs=[whole(pltpu.SMEM), whole(), whole()] + specs + specs,
        out_specs=pl.BlockSpec((seqs, rows, wide), lambda j: (0, 0, j)),
        out_shape=jax.ShapeDtypeStruct((seqs, rows, ny * wide), BF16),
        compiler_params=params(),
        name="finish",
    )(places, pooled, attn, *own, *other)


def after(x, *others):
    return lax.optimization_barrier((x,) + others)[0]


def placed(pieces, where, dim):
    shape = list(pieces[0].shape)
    shape[dim] = len(pieces)
    out = jnp.zeros(shape, pieces[0].dtype)
    for piece, at in zip(pieces, where):
        out = lax.dynamic_update_slice_in_dim(out, piece, at, dim)
    return out


def on_device(
    tokens,
    norm_gain,
    w_pool_in,
    pool_mix,
    pool_scale,
    w_query,
    w_key,
    w_value,
    gate_cache,
    w_out_pool,
    w_out_attn,
):
    z = lax.axis_index("sp")
    x = lax.axis_index("tp_0")
    y = lax.axis_index("fs")
    c = lax.axis_index("tp_1")
    planes = lax.axis_size("sp")
    chunks = lax.axis_size("tp_0")
    seqs, rows, _ = tokens.shape
    block = rows * chunks * 2
    seen = [x, (x + 3) % 4, (x + 1) % 4, (x + 2) % 4]
    deeps = [y, (y + 3) % 4, (y + 1) % 4, (y + 2) % 4]
    places = jnp.stack([c] + seen + deeps).astype(jnp.int32)

    deep = w_key.shape[0]
    gain = lax.dynamic_slice_in_dim(norm_gain, y * deep, deep, 0)
    all_rows = ring_of_four(tokens, "tp_0")
    weights = jnp.concatenate([w_key, w_value, w_query, w_pool_in], axis=1)
    weights = (weights.astype(F32) * gain[:, None]).astype(BF16)
    here = lax.dynamic_slice_in_dim(gate_cache[:, 0], z * block, block, 1)
    high = lax.reduce_precision(here, 8, 7)
    rest = here - high
    middle = lax.reduce_precision(rest, 8, 7)
    parts = jnp.stack([high, middle, rest - middle], axis=1).astype(BF16)
    parts = jnp.pad(parts, ((0, 0), (0, 5), (0, 0))).reshape(GATE_ROWS, block)
    own_w = ring_of_four(jnp.concatenate([weights, parts], axis=0), "fs")
    other_w = sibling(own_w[0])
    other_w = (other_w, sibling(jnp.concatenate(own_w[1:], axis=0)))

    (kv,) = project(places, all_rows, own_w, other_w, 0, (1.0, 1.0), False)
    kv_here = lax.all_to_all(kv, "tp_0", 0, 0, tiled=True)
    kv = lax.all_to_all(kv_here.reshape(planes, 2 * rows + GATE_ROWS, HD), "sp", 0, 0, tiled=True)
    qp = project(
        places, all_rows, own_w, other_w, 1, (HD**-0.5 * LOG2E, 1.0), True
    )
    got = [qp[0]]
    for piece, by in zip(qp[1:], (-1, 1, 2)):
        got.append(
            lax.ppermute(piece, "tp_0", [(i, (i + by) % 4) for i in range(4)])
        )
    came = [x, (x + 1) % 4, (x + 3) % 4, (x + 2) % 4]
    qp = placed(got, came, 1)

    q = after(qp[0].reshape(planes, rows, HD), kv)
    q = lax.all_to_all(q, "sp", 0, 0, tiled=True)
    pool_in = qp[1]
    total = planes * chunks * 2
    border = lax.ppermute(
        pool_in[:, :, :, rows - 16 :], SP_TP, [(i, i + 1) for i in range(total - 1)]
    )
    first = (z * block + (2 * x + c) * rows).reshape(1).astype(jnp.int32)
    pooled = pool(first, pool_in, border, pool_mix, pool_scale.reshape(-1, HD))

    kv_own = ring_of_four(kv, "tp_0")
    kv_other = sibling(kv)
    kv_other = (kv_other, sibling(jnp.concatenate(kv_own[1:], axis=0)))

    out_w = jnp.concatenate([w_out_pool, w_out_attn], axis=0)
    o = ring_in_three(after(out_w, own_w[1]), "fs")
    o = placed([w[None] for w in o], deeps, 0)
    out_near = hops(after(o, kv_here), "tp_0")

    attn = attend(places, q, kv_own, kv_other)
    out_near = lax.optimization_barrier((*out_near, attn))[:2]
    out_own = (o, *out_near, *relays(*out_near, "tp_0"))
    out_other = [sibling(piece) for piece in out_own[1:3]]
    out_other += [sibling(piece) for piece in out_own[3:]]
    out_other = [sibling(o)] + out_other
    attn = lax.all_to_all(attn, "sp", 0, 0, tiled=True)
    attn = attn.reshape(chunks, seqs, 2, rows, HD)
    return finish(places, pooled, attn, out_own, out_other)


def solution(mesh):
    torus = Mesh(
        mesh.devices.reshape(mesh.shape["sp"], mesh.shape["fs"], 4, 2), ("sp", "fs", "tp_0", "tp_1")
    )
    return jax.shard_map(
        on_device,
        mesh=torus,
        in_specs=(
            P("fs", SP_TP, None),
            P(),
            P("fs", TP),
            P(),
            P(),
            P("fs", TP),
            P("fs", TP),
            P("fs", TP),
            P("fs", TP, None),
            P(TP, "fs"),
            P(TP, "fs"),
        ),
        out_specs=P("fs", SP_TP, None),
        check_vma=False,
    )
```
